1024 devices in a mesh: tp: 128 (over z, y), dp: 8 (over x, core).
Axes of the slice: x: 4, y: 4, z: 32, core: 2. Of those that a mesh axis runs over, the one named last changes fastest.
Arguments:
- tokens: bfloat16 [64, 4096], P('dp', 'tp'), may hold values from -6 to 6
- norm_gain: float32 [2, 4096], replicated, may hold values from 0.1 to 1.9
- w_query: bfloat16 [2, 4096, 2048], P(None, 'dp', 'tp'), may hold values from -0.09375 to 0.09375
- w_key: bfloat16 [2, 4096, 2048], P(None, 'dp', 'tp'), may hold values from -0.09375 to 0.09375
- w_value: bfloat16 [2, 4096, 4096], P(None, 'dp', 'tp'), may hold values from -0.09375 to 0.09375
- w_outgate: bfloat16 [2, 4096, 4096], P(None, 'dp', 'tp'), may hold values from -0.09375 to 0.09375
- w_ingate: bfloat16 [2, 4096, 16], P(None, 'dp'), may hold values from -0.09375 to 0.09375
- w_forget: bfloat16 [2, 4096, 16], P(None, 'dp'), may hold values from -0.09375 to 0.09375
- forget_bias: float32 [2, 16], replicated, may hold values from -2 to 5
- w_output: bfloat16 [2, 4096, 4096], P(None, 'dp', 'tp'), may hold values from -0.09375 to 0.09375
- mem_state: float32 [2, 64, 4096, 128], P(None, 'dp', 'tp'), may hold values from -0.8 to 0.8
- norm_state: float32 [2, 64, 16, 128], P(None, 'dp'), may hold values from -0.8 to 0.8
- max_state: float32 [2, 64, 16], P(None, 'dp'), may hold values from -4 to 4
Outputs:
- mixed: bfloat16 [64, 4096], P('dp', 'tp')
- new_memory: float32 [2, 64, 4096, 128], P(None, 'dp', 'tp')
- new_normaliser: float32 [2, 64, 16, 128], P(None, 'dp')
- new_stabiliser: float32 [2, 64, 16], P(None, 'dp')
The draws below stay inside these ranges and needn't reach their ends.
All inputs are finite; a program needn't handle non-finite values.
Results may differ from the reference program's by a relative error of at most 0.013.
Values may be sent and summed in bfloat16 or wider, within the bound.
No kernel may reach another device: no remote copies, remote signals or barrier semaphores. Data moves between devices by JAX's collectives and lax.ppermute only.
A program may use at most 32 MiB of HBM per device.

```python
import jax
import jax.numpy as jnp
from jax import lax

D = 4096
H = 16
DK = 128
DV = 256
BLOCKS = 2
SEQS = 64


def levels(own_key, shape, split, least, top_value):
    def one(position, blocks):
        steps = jax.random.uniform(jax.random.fold_in(jax.random.fold_in(own_key, 6), position), (blocks,), jnp.float32, least / len(split), top_value / len(split))
        return jnp.repeat(jnp.exp(steps), shape[position] // blocks).reshape((-1,) + (1,) * (len(shape) - position - 1))

    level = one(*split[0])
    for cut in split[1:]:
        level = level * one(*cut)
    return level


def gaussian(own_key, dims, deviation, limit, cuts=(), dtype=jnp.bfloat16):
    entries = jax.random.normal(own_key, dims, jnp.float32) * deviation
    if len(cuts) > 0:
        entries = levels(own_key, dims, cuts, -0.22, 0.18) * entries
    return jnp.clip(entries, min=-limit, max=limit).astype(dtype)


def setup_inputs(seed: int = 0) -> dict:
    splits = jax.random.split(jax.random.key(seed), 14)
    return {
        "tokens": gaussian(splits[0], (SEQS, D), 1.0, 6.0, ((0, 8), (1, 128))),
        "norm_gain": jnp.clip(1.0 + 0.18 * jax.random.normal(splits[1], (BLOCKS, D), jnp.float32), 0.1, 1.9),
        "w_query": gaussian(splits[2], (BLOCKS, D, H * DK), D ** -0.5, 0.09375, ((1, 8), (2, 128))),
        "w_key": gaussian(splits[3], (BLOCKS, D, H * DK), D ** -0.5, 0.09375, ((1, 8), (2, 128))),
        "w_value": gaussian(splits[4], (BLOCKS, D, H * DV), D ** -0.5, 0.09375, ((1, 8), (2, 128))),
        "w_outgate": gaussian(splits[5], (BLOCKS, D, H * DV), D ** -0.5, 0.09375, ((1, 8), (2, 128))),
        "w_ingate": gaussian(splits[6], (BLOCKS, D, H), D ** -0.5, 0.09375, ((1, 8),)),
        "w_forget": gaussian(splits[7], (BLOCKS, D, H), D ** -0.5, 0.09375, ((1, 8),)),
        "forget_bias": jnp.clip(jax.random.uniform(splits[8], (BLOCKS, H), jnp.float32, -2.0, 5.0), -2.0, 5.0),
        "w_output": gaussian(splits[9], (BLOCKS, H * DV, D), (H * DV) ** -0.5, 0.09375, ((1, 8), (2, 128))),
        "mem_state": gaussian(splits[10], (BLOCKS, SEQS, H * DV, DK), 0.1, 0.8, ((1, 8), (2, 128)), jnp.float32),
        "norm_state": gaussian(splits[11], (BLOCKS, SEQS, H, DK), 0.1, 0.8, ((1, 8),), jnp.float32),
        "max_state": gaussian(splits[12], (BLOCKS, SEQS, H), 1.0, 4.0, ((1, 8),), jnp.float32),
    }


EPSILON = 1e-06

def mlstm_block(current, gain, w_query, w_key, w_value, w_outgate, w_ingate, w_forget, bias, w_output, memory, normaliser, stabiliser):
    seq_count = current.shape[0]
    wide = current.astype(jnp.float32)
    scale = lax.rsqrt(lax.optimization_barrier(jnp.mean(wide * wide, axis=-1, keepdims=True)) + EPSILON)
    normed = (wide * scale * gain).astype(jnp.bfloat16)
    query = jnp.dot(normed, w_query, preferred_element_type=jnp.float32).astype(jnp.bfloat16)
    keys = jnp.dot(normed, w_key, preferred_element_type=jnp.float32).astype(jnp.bfloat16)
    values = jnp.dot(normed, w_value, preferred_element_type=jnp.float32).astype(jnp.bfloat16)
    outgate = jnp.dot(normed, w_outgate, preferred_element_type=jnp.float32).astype(jnp.bfloat16)
    in_pre = jnp.dot(normed, w_ingate, preferred_element_type=jnp.float32)
    forget_pre = jnp.dot(normed, w_forget, preferred_element_type=jnp.float32)
    log_forget = jax.nn.log_sigmoid(forget_pre + bias)
    new_max = jnp.maximum(log_forget + stabiliser, in_pre)
    carried = jnp.exp(log_forget + stabiliser - new_max)
    fresh = jnp.exp(in_pre - new_max)
    query_heads = query.astype(jnp.float32).reshape(seq_count, H, DK)
    key_heads = keys.astype(jnp.float32).reshape(seq_count, H, DK) * DK ** (-0.5)
    value_heads = values.astype(jnp.float32).reshape(seq_count, H, DV)
    state = memory.reshape(seq_count, H, DV, DK)
    new_state = carried[:, :, None, None] * state + fresh[:, :, None, None] * value_heads[:, :, :, None] * key_heads[:, :, None, :]
    new_norm = carried[:, :, None] * normaliser + fresh[:, :, None] * key_heads
    divisor = jnp.maximum(jnp.abs(lax.optimization_barrier(jnp.sum(new_norm * query_heads, axis=-1))), 1.0)
    readout = lax.optimization_barrier(jnp.sum(new_state * query_heads[:, :, None, :], axis=-1)) / divisor[:, :, None]
    gated = (jax.nn.sigmoid(outgate.astype(jnp.float32)) * readout.reshape(seq_count, H * DV)).astype(jnp.bfloat16)
    update = jnp.dot(gated, w_output, preferred_element_type=jnp.float32)
    return ((wide + update).astype(jnp.bfloat16), new_state.reshape(seq_count, H * DV, DK), new_norm, new_max)

def reference(tokens, norm_gain, w_query, w_key, w_value, w_outgate, w_ingate, w_forget, forget_bias, w_output, mem_state, norm_state, max_state):
    current = tokens
    memories, normalisers, maxima = ([], [], [])
    for layer in range(BLOCKS):
        current, memory, normaliser, stabiliser = mlstm_block(current, norm_gain[layer], w_query[layer], w_key[layer], w_value[layer], w_outgate[layer], w_ingate[layer], w_forget[layer], forget_bias[layer], w_output[layer], mem_state[layer], norm_state[layer], max_state[layer])
        memories.append(memory)
        normalisers.append(normaliser)
        maxima.append(stabiliser)
    return (current, jnp.stack(memories), jnp.stack(normalisers), jnp.stack(maxima))
```

```python
import jax
import jax.numpy as jnp
from jax import lax
from jax.sharding import Mesh
from jax.sharding import PartitionSpec as P

H = 16
DK = 128
DV = 256
BLOCKS = 2
EPSILON = 1e-06

HEAD = ("zq", "y")
TP = ("h", "zq", "y")


def to_all(x, axes):
    size = lax.axis_size(axes)
    flat = x.reshape(1, -1, 128)
    sent = jnp.broadcast_to(flat, (size, *flat.shape[1:]))
    return lax.all_to_all(sent, axes, 0, 0, tiled=True)


def side_by_side(pieces):
    count, rows, cols = pieces.shape
    return pieces.transpose(1, 0, 2).reshape(rows, count * cols)


def rows_to_all(w):
    cols, rows = w.shape
    size = lax.axis_size("x")
    at = lax.axis_index("x")
    core = lax.axis_index("c")
    held = jnp.zeros((size, cols, rows), w.dtype)
    for k in range(size):
        piece = lax.ppermute(w, "x", [(i, (i + k) % size) for i in range(size)]) if k else w
        held = lax.dynamic_update_index_in_dim(held, piece, (at + size - k) % size, 0)
    other = lax.ppermute(held, "c", [(0, 1), (1, 0)])
    first = jnp.where(core == 0, held, other)
    second = jnp.where(core == 0, other, held)
    both = jnp.stack([first, second], axis=1)
    return both.transpose(2, 0, 1, 3).reshape(cols, 2 * size * rows)


def times(a, w):
    return lax.dot_general(a, w, (((1,), (1,)), ((), ())), preferred_element_type=jnp.float32)


def shards(
    tokens,
    norm_gain,
    w_query,
    w_key,
    w_value,
    w_outgate,
    w_ingate,
    w_forget,
    forget_bias,
    w_output,
    mem_state,
    norm_state,
    max_state,
):
    seqs, cols = tokens.shape
    key_cols = w_query.shape[2]
    head = lax.axis_index("h")
    projections = (w_query, w_key, w_value, w_outgate, w_ingate, w_forget)

    def lines(layer):
        return [w[layer].T for w in projections]

    wide_cols = sum(w.shape[2] for w in projections)
    with jax.named_scope("early_rows"):
        early = rows_to_all(jnp.concatenate([*lines(0), w_output[0].T, w_output[1].T]))
    with jax.named_scope("late_rows"):
        late = rows_to_all(jnp.concatenate(lines(1)))
    w_in = [early[:wide_cols], late]
    w_out = [early[wide_cols : wide_cols + cols], early[wide_cols + cols :]]

    current = tokens
    memories, normalisers, maxima = ([], [], [])
    for layer in range(BLOCKS):
        with jax.named_scope(f"mix_{layer}"):
            pieces = to_all(current, TP)
        whole = side_by_side(pieces.reshape(-1, seqs, cols))
        wide = whole.astype(jnp.float32)
        scale = lax.rsqrt(jnp.mean(wide * wide, axis=-1, keepdims=True) + EPSILON)
        normed = (wide * scale * norm_gain[layer]).astype(jnp.bfloat16)
        product = times(normed, w_in[layer])
        query_key = product[:, : 2 * key_cols].astype(jnp.bfloat16)
        keys_own = product[:, key_cols : 2 * key_cols].astype(jnp.bfloat16)
        at = 2 * key_cols
        values = product[:, at : at + cols].astype(jnp.bfloat16).astype(jnp.float32)
        outgate = product[:, at + cols : at + 2 * cols].astype(jnp.bfloat16).astype(jnp.float32)
        in_pre = product[:, at + 2 * cols : at + 2 * cols + H]
        forget_pre = product[:, at + 2 * cols + H :]
        log_forget = jax.nn.log_sigmoid(forget_pre + forget_bias[layer])
        new_max = jnp.maximum(log_forget + max_state[layer], in_pre)
        carried = jnp.exp(log_forget + max_state[layer] - new_max)
        fresh = jnp.exp(in_pre - new_max)

        with jax.named_scope(f"heads_{layer}"):
            pieces = to_all(query_key, HEAD).reshape(-1, seqs, 2, key_cols)
        query = side_by_side(pieces[:, :, 0]).astype(jnp.float32)
        key = side_by_side(pieces[:, :, 1]).astype(jnp.float32) * DK ** (-0.5)

        def own(x):
            return lax.dynamic_index_in_dim(x, head, axis=1, keepdims=False)

        carried_own = own(carried)
        fresh_own = own(fresh)
        norm_own = carried_own[:, None] * own(norm_state[layer]) + fresh_own[:, None] * key
        divisor = jnp.maximum(jnp.abs(jnp.sum(norm_own * query, axis=-1)), 1.0)
        new_state = (
            carried_own[:, None, None] * mem_state[layer]
            + (fresh_own[:, None] * values)[:, :, None] * key[:, None, :]
        )
        readout = jnp.sum(new_state * query[:, None, :], axis=-1) / divisor[:, None]
        gated = (jax.nn.sigmoid(outgate) * readout).astype(jnp.bfloat16)

        sent = jnp.concatenate([gated.reshape(-1), keys_own.reshape(-1)])
        with jax.named_scope(f"gated_{layer}"):
            got = to_all(sent, TP)
        split = seqs * cols // 128
        gated_all = side_by_side(got[:, :split].reshape(-1, seqs, cols))
        keys_all = side_by_side(got[:, split:].reshape(-1, seqs, key_cols))
        key_heads = keys_all.astype(jnp.float32).reshape(seqs, H, DK) * DK ** (-0.5)
        new_norm = carried[:, :, None] * norm_state[layer] + fresh[:, :, None] * key_heads
        update = times(gated_all, w_out[layer])
        current = (current.astype(jnp.float32) + update).astype(jnp.bfloat16)
        memories.append(new_state)
        normalisers.append(new_norm)
        maxima.append(new_max)
    return (current, jnp.stack(memories), jnp.stack(normalisers), jnp.stack(maxima))


def solution(mesh):
    dp = ("x", "c")
    split = Mesh(
        mesh.devices.reshape(16, 2, 4, mesh.shape["dp"] // 2, 2), ("h", "zq", "y", "x", "c")
    )
    return jax.shard_map(
        shards,
        mesh=split,
        in_specs=(
            P(dp, TP),
            P(),
            P(None, dp, TP),
            P(None, dp, TP),
            P(None, dp, TP),
            P(None, dp, TP),
            P(None, dp, None),
            P(None, dp, None),
            P(),
            P(None, dp, TP),
            P(None, dp, TP, None),
            P(None, dp, None, None),
            P(None, dp, None),
        ),
        out_specs=(
            P(dp, TP),
            P(None, dp, TP, None),
            P(None, dp, None, None),
            P(None, dp, None),
        ),
        check_vma=False,
    )
```

```python
import functools

import jax
import jax.numpy as jnp
from jax import lax
from jax.experimental import pallas as pl
from jax.experimental.pallas import tpu as pltpu
from jax.sharding import Mesh
from jax.sharding import PartitionSpec as P


H = 16
DK = 128
BLOCKS = 2
EPSILON = 1e-06
LANES = 128
SEG = 16
SEQS = 8

HEAD = ("zq", "y")
TP = ("h", "zq", "y")


def swap(x):
    x = x.reshape(-1, SEQS, LANES)
    row = lax.broadcasted_iota(jnp.int32, x.shape, 1)
    seg = lax.broadcasted_iota(jnp.int32, x.shape, 2) // SEG
    off = (seg - row + SEQS) % SEQS
    out = x
    for k in range(1, SEQS):
        moved = pltpu.roll(pltpu.roll(x, SEQS - k, 1), SEG * k, 2)
        out = jnp.where(off == k, moved, out)
    return out


def repeated(rows, count, ref):
    at = lax.broadcasted_iota(jnp.int32, rows.shape, 0) % count
    tile = jnp.broadcast_to(rows[0:1], rows.shape)
    for i in range(1, count):
        tile = jnp.where(at == i, jnp.broadcast_to(rows[i : i + 1], rows.shape), tile)
    tile = tile.astype(jnp.bfloat16)
    ref[...] = jnp.concatenate([tile] * (ref.shape[0] // SEQS), axis=0)


def rounded(x):
    return x.astype(jnp.bfloat16).astype(jnp.float32)


def contracted(place, wide, held, other, low, high):
    x, core = place[0], place[1]
    slots = held.shape[0]
    per = held.shape[2] // LANES
    total = None
    for k in range(slots):
        chip = lax.rem(x - k + slots, slots) * 2
        for ref, block in ((held, chip + core), (other, chip + 1 - core)):
            part = wide[pl.ds(block * per, per)].astype(jnp.bfloat16)
            lhs = jnp.concatenate([part[i] for i in range(per)], axis=1)
            term = lax.dot_general(
                lhs, ref[k, low:high, :], (((1,), (1,)), ((), ())), preferred_element_type=jnp.float32
            )
            total = term if total is None else total + term
    return total


def project_kernel(
    place, pieces, gain, held, other, bias, max_state, sent, product, new_max, carried, fresh, wide
):
    x = swap(pieces[...].astype(jnp.float32))
    count = x.shape[0]
    squares = jnp.sum(jnp.sum(x * x, axis=0), axis=1, keepdims=True)
    scale = lax.rsqrt(squares / (count * LANES) + EPSILON)
    wide[...] = x * scale[None] * gain[...][:, None, :]
    total = contracted(place, wide, held, other, 0, LANES)
    product[...] = total
    repeated(swap(total)[0], 2, sent)
    in_pre = total[:, LANES - 2 * H : LANES - H]
    forget = total[:, LANES - H :] + bias[...]
    log_forget = jnp.minimum(forget, 0.0) - jnp.log1p(jnp.exp(-jnp.abs(forget)))
    kept = log_forget + max_state[...]
    top = jnp.maximum(kept, in_pre)
    new_max[...] = top
    carried[...] = jnp.exp(kept - top)
    fresh[...] = jnp.exp(in_pre - top)


def state_kernel(*refs, last):
    if last:
        place, pieces, product, first, carried, fresh, norm, mem, _, new_mem, sent, rows = refs
    else:
        place, pieces, product, carried, fresh, norm, mem, new_mem, sent, rows = refs
    rows[...] = pieces[...].astype(jnp.float32)
    query = swap(rows[pl.ds(0, SEQS, stride=2), :])[0]
    key = swap(rows[pl.ds(1, SEQS, stride=2), :])[0] * DK ** (-0.5)
    head = place[2]
    mine = lax.broadcasted_iota(jnp.int32, (SEQS, H), 1) == head
    carry = jnp.sum(jnp.where(mine, carried[...], 0.0), axis=1, keepdims=True)
    new = jnp.sum(jnp.where(mine, fresh[...], 0.0), axis=1, keepdims=True)
    old = norm[0]
    at = lax.broadcasted_iota(jnp.int32, old.shape, 1) == head
    norm_own = carry * jnp.sum(jnp.where(at, old, 0.0), axis=1) + new * key
    divisor = jnp.maximum(jnp.abs(jnp.sum(norm_own * query, axis=1, keepdims=True)), 1.0)
    total = product[...]
    added = (rounded(total) * new).T
    cols = mem.shape[2]
    lane = lax.broadcasted_iota(jnp.int32, (cols, LANES), 1)
    read = jnp.zeros((cols, LANES), jnp.float32)
    for s in range(SEQS):
        state = carry[s : s + 1] * mem[0, s] + added[2 * SEG : 2 * SEG + cols, s : s + 1] * key[s : s + 1]
        new_mem[0, s] = state
        read = jnp.where(lane == s, jnp.sum(state * query[s : s + 1], axis=1, keepdims=True), read)
    square = jnp.concatenate([read, jnp.zeros((LANES - cols, LANES), jnp.float32)], axis=0)
    readout = square.T[:SEQS] / divisor
    gate = pltpu.roll(rounded(total), LANES - 2 * SEG - cols, 1)
    gated = jax.nn.sigmoid(gate) * readout
    lanes = lax.broadcasted_iota(jnp.int32, gated.shape, 1)
    row = jnp.where(lanes < cols, gated, pltpu.roll(total, SEG, 1))
    if last:
        row = jnp.where(lanes < cols + SEG, row, pltpu.roll(first[...], 2 * SEG, 1))
    repeated(swap(row)[0], 4 if last else 2, sent)


def output_kernel(place, pieces, held, other, x, new_x, sent, wide):
    wide[...] = swap(pieces[...].astype(jnp.float32))
    update = contracted(place, wide, held, other, LANES, LANES + x.shape[1])
    total = (x[...].astype(jnp.float32) + update).astype(jnp.bfloat16)
    new_x[...] = total
    room = jnp.zeros((SEQS, LANES - x.shape[1]), jnp.float32)
    repeated(swap(jnp.concatenate([total.astype(jnp.float32), room], axis=1))[0], 2, sent)


def final_kernel(
    place, pieces, held, other, x, carried0, fresh0, carried1, fresh1, norm, new_x, new_norm, rows, gathered, wide
):
    rows[...] = pieces[...].astype(jnp.float32)
    count = rows.shape[0] // 4
    for r in range(2):
        gathered[pl.ds(r, count, stride=2), :] = rows[pl.ds(r, count, stride=4), :]
    wide[...] = swap(gathered[...])
    low = LANES + x.shape[1]
    update = contracted(place, wide, held, other, low, low + x.shape[1])
    new_x[...] = (x[...].astype(jnp.float32) + update).astype(jnp.bfloat16)
    for layer, (carried, fresh) in enumerate(((carried0, fresh0), (carried1, fresh1))):
        keys = swap(rows[pl.ds(3 - layer, count, stride=4), :]) * DK ** (-0.5)
        for h in range(H):
            new_norm[layer, :, h, :] = (
                carried[:, h : h + 1] * norm[layer, :, h, :] + fresh[:, h : h + 1] * keys[h]
            )


SMEM = pl.BlockSpec(memory_space=pltpu.SMEM)
VMEM = pl.BlockSpec(memory_space=pltpu.VMEM)


def f32(*shape):
    return jax.ShapeDtypeStruct(shape, jnp.float32)


def bf16(*shape):
    return jax.ShapeDtypeStruct(shape, jnp.bfloat16)


def layer_block(shape, layer):
    return pl.BlockSpec((1, *shape[1:]), lambda i: (layer,) + (0,) * (len(shape) - 1))


def room():
    return pltpu.CompilerParams(vmem_limit_bytes=12 << 20)


def cost(flops):
    return pl.CostEstimate(flops=flops, bytes_accessed=1 << 20, transcendentals=0)


def project(place, pieces, gain, held, other, bias, max_state):
    tall = pieces.shape[0] // SEQS
    return pl.pallas_call(
        project_kernel,
        out_shape=(bf16(16, LANES), f32(SEQS, LANES), *[f32(SEQS, H)] * 3),
        in_specs=[SMEM] + [VMEM] * 6,
        out_specs=[VMEM] * 5,
        scratch_shapes=[pltpu.VMEM((tall, SEQS, LANES), jnp.float32)],
        compiler_params=room(),
        cost_estimate=cost(1 << 23),
        name="project",
    )(place, pieces, gain.reshape(tall, LANES), held, other, bias.reshape(1, H), max_state)


def renew(layer, place, pieces, product, first, carried, fresh, norm, mem, new_mem, devices):
    last = new_mem is not None
    args = [place, pieces, product] + ([first] if last else []) + [carried, fresh, norm, mem]
    whole = lambda a: pl.BlockSpec(a.shape, lambda i: (0,) * a.ndim)
    specs = [SMEM] + [whole(a) for a in args[1:-2]] + [layer_block(norm.shape, layer), layer_block(mem.shape, layer)]
    aliases = {}
    if last:
        aliases = {len(args): 0}
        args.append(new_mem)
        specs.append(pl.BlockSpec(memory_space=pl.ANY))
    rows = (4 if last else 2) * devices
    return pl.pallas_call(
        functools.partial(state_kernel, last=last),
        grid=(1,),
        out_shape=(f32(*mem.shape), bf16(rows, LANES)),
        in_specs=specs,
        out_specs=(layer_block(mem.shape, layer), pl.BlockSpec((rows, LANES), lambda i: (0, 0))),
        scratch_shapes=[pltpu.VMEM((2 * SEQS, LANES), jnp.float32)],
        input_output_aliases=aliases,
        compiler_params=room(),
        cost_estimate=cost(1 << 23),
        name="renew_last" if last else "renew",
    )(*args)


def output(place, pieces, held, other, x):
    return pl.pallas_call(
        output_kernel,
        out_shape=(bf16(*x.shape), bf16(*pieces.shape)),
        in_specs=[SMEM] + [VMEM] * 4,
        out_specs=[VMEM] * 2,
        scratch_shapes=[pltpu.VMEM((pieces.shape[0] // SEQS, SEQS, LANES), jnp.float32)],
        compiler_params=room(),
        cost_estimate=cost(1 << 23),
        name="output",
    )(place, pieces, held, other, x)


def final(place, pieces, held, other, x, gates, norm):
    half = pieces.shape[0] // 2
    return pl.pallas_call(
        final_kernel,
        out_shape=(bf16(*x.shape), f32(*norm.shape)),
        in_specs=[SMEM] + [VMEM] * 9,
        out_specs=[VMEM] * 2,
        scratch_shapes=[
            pltpu.VMEM((2 * half, LANES), jnp.float32),
            pltpu.VMEM((half, LANES), jnp.float32),
            pltpu.VMEM((half // SEQS, SEQS, LANES), jnp.float32),
        ],
        compiler_params=room(),
        cost_estimate=cost(1 << 23),
        name="final",
    )(place, pieces, held, other, x, *gates[0], *gates[1], norm)


def first_rows(x, devices):
    message = x.reshape(SEQS, -1, SEG).transpose(1, 0, 2).reshape(1, -1, LANES)
    return jnp.broadcast_to(message, (devices, *message.shape[1:])).reshape(-1, LANES)


def to_all(sent, axes):
    size = lax.axis_size(axes)
    got = lax.all_to_all(sent.reshape(size, -1, LANES), axes, 0, 0, tiled=True)
    return got.reshape(-1, LANES)


def rows_to_all(w):
    size = lax.axis_size("x")
    got = [
        lax.ppermute(w, "x", [(i, (i + k) % size) for i in range(size)]) for k in range(1, size)
    ]
    held = jnp.stack([w, *got])
    other = lax.ppermute(held, "c", [(0, 1), (1, 0)])
    return held, other


def shards(
    tokens,
    norm_gain,
    w_query,
    w_key,
    w_value,
    w_outgate,
    w_ingate,
    w_forget,
    forget_bias,
    w_output,
    mem_state,
    norm_state,
    max_state,
):
    devices = lax.axis_size(TP)
    place = jnp.stack([lax.axis_index("x"), lax.axis_index("c"), lax.axis_index("h")]).astype(jnp.int32)
    projections = (w_query, w_key, w_value, w_outgate, w_ingate, w_forget)

    def lines(layer):
        return [w[layer].T for w in projections]

    weights = [
        rows_to_all(jnp.concatenate([*lines(0), w_output[0].T, w_output[1].T])), rows_to_all(jnp.concatenate(lines(1)))
    ]
    current = tokens
    sent = first_rows(tokens, devices)
    gates, maxima, new_mem, first = ([], [], None, None)
    for layer in range(BLOCKS):
        pieces = to_all(sent, TP)
        sent, product, new_max, carried, fresh = project(
            place, pieces, norm_gain[layer], *weights[layer], forget_bias[layer], max_state[layer]
        )
        pieces = to_all(sent, HEAD)
        new_mem, sent = renew(
            layer, place, pieces, product, first, carried, fresh, norm_state, mem_state, new_mem, devices
        )
        first = product
        gates.append((carried, fresh))
        maxima.append(new_max)
        pieces = to_all(sent, TP)
        if layer < BLOCKS - 1:
            current, sent = output(place, pieces, *weights[0], current)
    current, new_norm = final(place, pieces, *weights[0], current, gates, norm_state)
    return (current, new_mem, new_norm, jnp.stack(maxima))


def solution(mesh):
    dp = ("x", "c")
    split = Mesh(
        mesh.devices.reshape(16, 2, 4, mesh.shape["dp"] // 2, 2), ("h", "zq", "y", "x", "c")
    )

    return jax.shard_map(
        shards,
        mesh=split,
        in_specs=(
            P(dp, TP),
            P(),
            P(None, dp, TP),
            P(None, dp, TP),
            P(None, dp, TP),
            P(None, dp, TP),
            P(None, dp, None),
            P(None, dp, None),
            P(),
            P(None, dp, TP),
            P(None, dp, TP, None),
            P(None, dp, None, None),
            P(None, dp, None),
        ),
        out_specs=(
            P(dp, TP),
            P(None, dp, TP, None),
            P(None, dp, None, None),
            P(None, dp, None),
        ),
        check_vma=False,
    )
```

```python
import functools

import jax
import jax.numpy as jnp
from jax import lax
from jax.experimental import pallas as pl
from jax.experimental.pallas import tpu as pltpu
from jax.sharding import Mesh
from jax.sharding import PartitionSpec as P


H = 16
DK = 128
DV = 256
BLOCKS = 2
EPSILON = 1e-06
LANES = 128
SEG = 16
SEQS = 8

HEAD = ("zq", "y")
TP = ("h", "zq", "y")


def swap(x):
    x = x.reshape(-1, SEQS, LANES)
    row = lax.broadcasted_iota(jnp.int32, x.shape, 1)
    seg = lax.broadcasted_iota(jnp.int32, x.shape, 2) // SEG
    off = (seg - row + SEQS) % SEQS
    out = x
    for k in range(1, SEQS):
        moved = pltpu.roll(pltpu.roll(x, SEQS - k, 1), SEG * k, 2)
        out = jnp.where(off == k, moved, out)
    return out


def repeated(rows, count, ref):
    at = lax.broadcasted_iota(jnp.int32, rows.shape, 0) % count
    tile = jnp.broadcast_to(rows[0:1], rows.shape)
    for i in range(1, count):
        tile = jnp.where(at == i, jnp.broadcast_to(rows[i : i + 1], rows.shape), tile)
    tile = tile.astype(jnp.bfloat16)
    ref[...] = jnp.concatenate([tile] * (ref.shape[0] // SEQS), axis=0)


def rounded(x):
    return x.astype(jnp.bfloat16).astype(jnp.float32)


def contracted(place, wide, held, other, low, high):
    x, core = place[0], place[1]
    slots = held.shape[0]
    per = held.shape[2] // LANES
    total = None
    for k in range(slots):
        chip = lax.rem(x - k + slots, slots) * 2
        for ref, block in ((held, chip + core), (other, chip + 1 - core)):
            part = wide[pl.ds(block * per, per)].astype(jnp.bfloat16)
            lhs = jnp.concatenate([part[i] for i in range(per)], axis=1)
            term = lax.dot_general(
                lhs, ref[k, low:high, :], (((1,), (1,)), ((), ())), preferred_element_type=jnp.float32
            )
            total = term if total is None else total + term
    return total


def prepare_kernel(*refs):
    x, sent, lines, sems = refs[0], refs[-3], refs[-2], refs[-1]
    weights, w_out = refs[1:-4], refs[-4]
    order = [(w, 0) for w in weights] + [(w_out, b) for b in range(BLOCKS)] + [(w, 1) for w in weights]
    copies, at = ([], 0)
    for i, (w, layer) in enumerate(order):
        copies.append(
            pltpu.make_async_copy(w.at[layer], lines.at[pl.ds(at, w.shape[1])], sems.at[i])
        )
        at += w.shape[1]
    for copy in copies:
        copy.start()
    room = jnp.zeros((SEQS, LANES - x.shape[1]), jnp.float32)
    repeated(swap(jnp.concatenate([x[...].astype(jnp.float32), room], axis=1))[0], 2, sent)
    for copy in copies:
        copy.wait()


def project_kernel(
    place, pieces, gain, held, other, bias, max_state, sent, product, new_max, carried, fresh, wide, *, low
):
    x = swap(pieces[...].astype(jnp.float32))
    count = x.shape[0]
    squares = jnp.sum(jnp.sum(x * x, axis=0), axis=1, keepdims=True)
    scale = lax.rsqrt(squares / (count * LANES) + EPSILON)
    wide[...] = x * scale[None] * gain[...][:, None, :]
    total = contracted(place, wide, held, other, low, low + LANES)
    product[...] = total
    repeated(swap(total)[0], 2, sent)
    in_pre = total[:, LANES - 2 * H : LANES - H]
    forget = total[:, LANES - H :] + bias[...]
    log_forget = jnp.minimum(forget, 0.0) - jnp.log1p(jnp.exp(-jnp.abs(forget)))
    kept = log_forget + max_state[...]
    top = jnp.maximum(kept, in_pre)
    new_max[...] = top
    carried[...] = jnp.exp(kept - top)
    fresh[...] = jnp.exp(in_pre - top)


def state_kernel(*refs, last):
    if last:
        place, pieces, product, first, carried, fresh, norm, mem, _, new_mem, sent, rows = refs
    else:
        place, pieces, product, carried, fresh, norm, mem, new_mem, sent, rows = refs
    rows[...] = pieces[...].astype(jnp.float32)
    query = swap(rows[pl.ds(0, SEQS, stride=2), :])[0]
    key = swap(rows[pl.ds(1, SEQS, stride=2), :])[0] * DK ** (-0.5)
    head = place[2]
    mine = lax.broadcasted_iota(jnp.int32, (SEQS, H), 1) == head
    carry = jnp.sum(jnp.where(mine, carried[...], 0.0), axis=1, keepdims=True)
    new = jnp.sum(jnp.where(mine, fresh[...], 0.0), axis=1, keepdims=True)
    old = norm[0]
    at = lax.broadcasted_iota(jnp.int32, old.shape, 1) == head
    norm_own = carry * jnp.sum(jnp.where(at, old, 0.0), axis=1) + new * key
    divisor = jnp.maximum(jnp.abs(jnp.sum(norm_own * query, axis=1, keepdims=True)), 1.0)
    total = product[...]
    added = (rounded(total) * new).T
    cols = mem.shape[2]
    lane = lax.broadcasted_iota(jnp.int32, (cols, LANES), 1)
    read = jnp.zeros((cols, LANES), jnp.float32)
    for s in range(SEQS):
        state = carry[s : s + 1] * mem[0, s] + added[2 * SEG : 2 * SEG + cols, s : s + 1] * key[s : s + 1]
        new_mem[0, s] = state
        read = jnp.where(lane == s, jnp.sum(state * query[s : s + 1], axis=1, keepdims=True), read)
    square = jnp.concatenate([read, jnp.zeros((LANES - cols, LANES), jnp.float32)], axis=0)
    readout = square.T[:SEQS] / divisor
    gate = pltpu.roll(rounded(total), LANES - 2 * SEG - cols, 1)
    gated = jax.nn.sigmoid(gate) * readout
    lanes = lax.broadcasted_iota(jnp.int32, gated.shape, 1)
    row = jnp.where(lanes < cols, gated, pltpu.roll(total, SEG, 1))
    if last:
        row = jnp.where(lanes < cols + SEG, row, pltpu.roll(first[...], 2 * SEG, 1))
    repeated(swap(row)[0], 4 if last else 2, sent)


def output_kernel(place, pieces, held, other, x, new_x, sent, wide):
    wide[...] = swap(pieces[...].astype(jnp.float32))
    update = contracted(place, wide, held, other, LANES, LANES + x.shape[1])
    total = (x[...].astype(jnp.float32) + update).astype(jnp.bfloat16)
    new_x[...] = total
    room = jnp.zeros((SEQS, LANES - x.shape[1]), jnp.float32)
    repeated(swap(jnp.concatenate([total.astype(jnp.float32), room], axis=1))[0], 2, sent)


def final_kernel(
    place, pieces, held, other, x, carried0, fresh0, carried1, fresh1, norm, max0, max1,
    new_x, new_norm, new_max, rows, gathered, wide,
):
    new_max[0] = max0[...]
    new_max[1] = max1[...]
    rows[...] = pieces[...].astype(jnp.float32)
    count = rows.shape[0] // 4
    for r in range(2):
        gathered[pl.ds(r, count, stride=2), :] = rows[pl.ds(r, count, stride=4), :]
    wide[...] = swap(gathered[...])
    low = LANES + x.shape[1]
    update = contracted(place, wide, held, other, low, low + x.shape[1])
    new_x[...] = (x[...].astype(jnp.float32) + update).astype(jnp.bfloat16)
    for layer, (carried, fresh) in enumerate(((carried0, fresh0), (carried1, fresh1))):
        keys = swap(rows[pl.ds(3 - layer, count, stride=4), :]) * DK ** (-0.5)
        for h in range(H):
            new_norm[layer, :, h, :] = (
                carried[:, h : h + 1] * norm[layer, :, h, :] + fresh[:, h : h + 1] * keys[h]
            )


SMEM = pl.BlockSpec(memory_space=pltpu.SMEM)
VMEM = pl.BlockSpec(memory_space=pltpu.VMEM)


def f32(*shape):
    return jax.ShapeDtypeStruct(shape, jnp.float32)


def bf16(*shape):
    return jax.ShapeDtypeStruct(shape, jnp.bfloat16)


def layer_block(shape, layer):
    return pl.BlockSpec((1, *shape[1:]), lambda i: (layer,) + (0,) * (len(shape) - 1))


def room(mib=12):
    return pltpu.CompilerParams(vmem_limit_bytes=mib << 20)


def cost(flops):
    return pl.CostEstimate(flops=flops, bytes_accessed=1 << 20, transcendentals=0)


def prepare(x, projections, w_output, devices):
    args = [x, *[w.transpose(0, 2, 1) for w in projections], w_output.transpose(0, 2, 1)]
    rows = args[1].shape[2]
    cols = sum(w.shape[0] * w.shape[1] for w in args[1:])
    return pl.pallas_call(
        prepare_kernel,
        out_shape=(bf16(2 * devices, LANES), bf16(cols, rows)),
        in_specs=[VMEM] + [pl.BlockSpec(memory_space=pltpu.HBM)] * (len(args) - 1),
        out_specs=[VMEM] * 2,
        scratch_shapes=[pltpu.SemaphoreType.DMA((2 * len(projections) + BLOCKS,))],
        compiler_params=room(60),
        cost_estimate=cost(1 << 23),
        name="prepare",
    )(*args)


def project(layer, place, pieces, gain, held, other, bias, max_state):
    tall = pieces.shape[0] // SEQS
    low = (LANES + 2 * DV // SEQS) * layer
    return pl.pallas_call(
        functools.partial(project_kernel, low=low),
        out_shape=(bf16(16, LANES), f32(SEQS, LANES), *[f32(SEQS, H)] * 3),
        in_specs=[SMEM] + [VMEM] * 6,
        out_specs=[VMEM] * 5,
        scratch_shapes=[pltpu.VMEM((tall, SEQS, LANES), jnp.float32)],
        compiler_params=room(),
        cost_estimate=cost(1 << 23),
        name="project",
    )(place, pieces, gain.reshape(tall, LANES), held, other, bias.reshape(1, H), max_state)


def renew(layer, place, pieces, product, first, carried, fresh, norm, mem, new_mem, devices):
    last = new_mem is not None
    args = [place, pieces, product] + ([first] if last else []) + [carried, fresh, norm, mem]
    whole = lambda a: pl.BlockSpec(a.shape, lambda i: (0,) * a.ndim)
    specs = [SMEM] + [whole(a) for a in args[1:-2]] + [layer_block(norm.shape, layer), layer_block(mem.shape, layer)]
    aliases = {}
    if last:
        aliases = {len(args): 0}
        args.append(new_mem)
        specs.append(pl.BlockSpec(memory_space=pl.ANY))
    rows = (4 if last else 2) * devices
    return pl.pallas_call(
        functools.partial(state_kernel, last=last),
        grid=(1,),
        out_shape=(f32(*mem.shape), bf16(rows, LANES)),
        in_specs=specs,
        out_specs=(layer_block(mem.shape, layer), pl.BlockSpec((rows, LANES), lambda i: (0, 0))),
        scratch_shapes=[pltpu.VMEM((2 * SEQS, LANES), jnp.float32)],
        input_output_aliases=aliases,
        compiler_params=room(),
        cost_estimate=cost(1 << 23),
        name="renew_last" if last else "renew",
    )(*args)


def output(place, pieces, held, other, x):
    return pl.pallas_call(
        output_kernel,
        out_shape=(bf16(*x.shape), bf16(*pieces.shape)),
        in_specs=[SMEM] + [VMEM] * 4,
        out_specs=[VMEM] * 2,
        scratch_shapes=[pltpu.VMEM((pieces.shape[0] // SEQS, SEQS, LANES), jnp.float32)],
        compiler_params=room(),
        cost_estimate=cost(1 << 23),
        name="output",
    )(place, pieces, held, other, x)


def final(place, pieces, held, other, x, gates, norm, maxima):
    half = pieces.shape[0] // 2
    return pl.pallas_call(
        final_kernel,
        out_shape=(bf16(*x.shape), f32(*norm.shape), f32(BLOCKS, SEQS, H)),
        in_specs=[SMEM] + [VMEM] * 11,
        out_specs=[VMEM] * 3,
        scratch_shapes=[
            pltpu.VMEM((2 * half, LANES), jnp.float32),
            pltpu.VMEM((half, LANES), jnp.float32),
            pltpu.VMEM((half // SEQS, SEQS, LANES), jnp.float32),
        ],
        compiler_params=room(),
        cost_estimate=cost(1 << 23),
        name="final",
    )(place, pieces, held, other, x, *gates[0], *gates[1], norm, *maxima)


def to_all(sent, axes):
    size = lax.axis_size(axes)
    got = lax.all_to_all(sent.reshape(size, -1, LANES), axes, 0, 0, tiled=True)
    return got.reshape(-1, LANES)


def rows_to_all(w):
    size = lax.axis_size("x")
    got = [
        lax.ppermute(w, "x", [(i, (i + k) % size) for i in range(size)]) for k in range(1, size)
    ]
    held = jnp.stack([w, *got])
    other = lax.ppermute(held, "c", [(0, 1), (1, 0)])
    return held, other


def shards(
    tokens,
    norm_gain,
    w_query,
    w_key,
    w_value,
    w_outgate,
    w_ingate,
    w_forget,
    forget_bias,
    w_output,
    mem_state,
    norm_state,
    max_state,
):
    devices = lax.axis_size(TP)
    place = jnp.stack([lax.axis_index("x"), lax.axis_index("c"), lax.axis_index("h")]).astype(jnp.int32)
    projections = (w_query, w_key, w_value, w_outgate, w_ingate, w_forget)

    sent, lines = prepare(tokens, projections, w_output, devices)
    weights = rows_to_all(lines)
    current = tokens
    gates, maxima, new_mem, first = ([], [], None, None)
    for layer in range(BLOCKS):
        pieces = to_all(sent, TP)
        sent, product, new_max, carried, fresh = project(
            layer, place, pieces, norm_gain[layer], *weights, forget_bias[layer], max_state[layer]
        )
        pieces = to_all(sent, HEAD)
        new_mem, sent = renew(
            layer, place, pieces, product, first, carried, fresh, norm_state, mem_state, new_mem, devices
        )
        first = product
        gates.append((carried, fresh))
        maxima.append(new_max)
        pieces = to_all(sent, TP)
        if layer < BLOCKS - 1:
            current, sent = output(place, pieces, *weights, current)
    current, new_norm, new_max = final(place, pieces, *weights, current, gates, norm_state, maxima)
    return (current, new_mem, new_norm, new_max)


def solution(mesh):
    dp = ("x", "c")
    split = Mesh(
        mesh.devices.reshape(16, 2, 4, mesh.shape["dp"] // 2, 2), ("h", "zq", "y", "x", "c")
    )

    return jax.shard_map(
        shards,
        mesh=split,
        in_specs=(
            P(dp, TP),
            P(),
            P(None, dp, TP),
            P(None, dp, TP),
            P(None, dp, TP),
            P(None, dp, TP),
            P(None, dp, None),
            P(None, dp, None),
            P(),
            P(None, dp, TP),
            P(None, dp, TP, None),
            P(None, dp, None, None),
            P(None, dp, None),
        ),
        out_specs=(
            P(dp, TP),
            P(None, dp, TP, None),
            P(None, dp, None, None),
            P(None, dp, None),
        ),
        check_vma=False,
    )
```

```python
import functools

import jax
import jax.numpy as jnp
from jax import lax
from jax.experimental import pallas as pl
from jax.experimental.pallas import tpu as pltpu
from jax.sharding import Mesh
from jax.sharding import PartitionSpec as P


H = 16
DK = 128
DV = 256
BLOCKS = 2
EPSILON = 1e-06
LANES = 128
SEG = 16
SEQS = 8

PER_HEAD = 8
TURN = 2


def swap(x):
    x = x.reshape(-1, SEQS, LANES)
    row = lax.broadcasted_iota(jnp.int32, x.shape, 1)
    seg = lax.broadcasted_iota(jnp.int32, x.shape, 2) // SEG
    off = (seg - row + SEQS) % SEQS
    out = x
    for k in range(1, SEQS):
        moved = pltpu.roll(pltpu.roll(x, SEQS - k, 1), SEG * k, 2)
        out = jnp.where(off == k, moved, out)
    return out


def repeated(rows, count, ref):
    at = lax.broadcasted_iota(jnp.int32, rows.shape, 0) % count
    tile = jnp.broadcast_to(rows[0:1], rows.shape)
    for i in range(1, count):
        tile = jnp.where(at == i, jnp.broadcast_to(rows[i : i + 1], rows.shape), tile)
    tile = tile.astype(jnp.bfloat16)
    ref[...] = jnp.concatenate([tile] * (ref.shape[0] // SEQS), axis=0)


def rounded(x):
    return x.astype(jnp.bfloat16).astype(jnp.float32)


def contracted(place, wide, held, other, low, high):
    x, core = place[0], place[1]
    slots = held.shape[0]
    per = held.shape[2] // LANES
    total = None
    for k in range(slots):
        chip = lax.rem(x - k + slots, slots) * 2
        for ref, block in ((held, chip + core), (other, chip + 1 - core)):
            block = lax.rem(block + slots, 2 * slots)
            part = wide[pl.ds(block * per, per)].astype(jnp.bfloat16)
            lhs = jnp.concatenate([part[i] for i in range(per)], axis=1)
            term = lax.dot_general(
                lhs, ref[k, low:high, :], (((1,), (1,)), ((), ())), preferred_element_type=jnp.float32
            )
            total = term if total is None else total + term
    return total


def prepare_kernel(*refs):
    x, sent, lines, sems = refs[0], refs[-3], refs[-2], refs[-1]
    weights, w_out = refs[1:-4], refs[-4]
    order = [(w, 0) for w in weights] + [(w_out, b) for b in range(BLOCKS)] + [(w, 1) for w in weights]
    copies, at = ([], 0)
    for i, (w, layer) in enumerate(order):
        copies.append(
            pltpu.make_async_copy(w.at[layer], lines.at[pl.ds(at, w.shape[1])], sems.at[i])
        )
        at += w.shape[1]
    for copy in copies:
        copy.start()
    room = jnp.zeros((SEQS, LANES - x.shape[1]), jnp.float32)
    repeated(swap(jnp.concatenate([x[...].astype(jnp.float32), room], axis=1))[0], 2, sent)
    for copy in copies:
        copy.wait()


def project_kernel(
    place, pieces, gain, held, other, bias, max_state, sent, product, new_max, carried, fresh, wide, *, low
):
    x = swap(pieces[...].astype(jnp.float32))
    count = x.shape[0]
    squares = jnp.sum(jnp.sum(x * x, axis=0), axis=1, keepdims=True)
    scale = lax.rsqrt(squares / (count * LANES) + EPSILON)
    turned = jnp.concatenate([gain[count // TURN :], gain[: count // TURN]], axis=0)
    wide[...] = x * scale[None] * turned[:, None, :]
    total = contracted(place, wide, held, other, low, low + LANES)
    product[...] = total
    repeated(swap(total)[0], 2, sent)
    in_pre = total[:, LANES - 2 * H : LANES - H]
    forget = total[:, LANES - H :] + bias[...]
    log_forget = jnp.minimum(forget, 0.0) - jnp.log1p(jnp.exp(-jnp.abs(forget)))
    kept = log_forget + max_state[...]
    top = jnp.maximum(kept, in_pre)
    new_max[...] = top
    carried[...] = jnp.exp(kept - top)
    fresh[...] = jnp.exp(in_pre - top)


def state_kernel(*refs, last):
    if last:
        place, pieces, product, first, carried, fresh, norm, mem, _, new_mem, sent, rows = refs
    else:
        place, pieces, product, carried, fresh, norm, mem, new_mem, sent, rows = refs
    rows[...] = pieces[...].astype(jnp.float32)
    query = swap(rows[pl.ds(0, SEQS, stride=2), :])[0]
    key = swap(rows[pl.ds(1, SEQS, stride=2), :])[0] * DK ** (-0.5)
    head = place[2]
    mine = lax.broadcasted_iota(jnp.int32, (SEQS, H), 1) == head
    carry = jnp.sum(jnp.where(mine, carried[...], 0.0), axis=1, keepdims=True)
    new = jnp.sum(jnp.where(mine, fresh[...], 0.0), axis=1, keepdims=True)
    old = norm[0]
    at = lax.broadcasted_iota(jnp.int32, old.shape, 1) == head
    norm_own = carry * jnp.sum(jnp.where(at, old, 0.0), axis=1) + new * key
    divisor = jnp.maximum(jnp.abs(jnp.sum(norm_own * query, axis=1, keepdims=True)), 1.0)
    total = product[...]
    added = (rounded(total) * new).T
    cols = mem.shape[2]
    lane = lax.broadcasted_iota(jnp.int32, (cols, LANES), 1)
    read = jnp.zeros((cols, LANES), jnp.float32)
    for s in range(SEQS):
        state = carry[s : s + 1] * mem[0, s] + added[2 * SEG : 2 * SEG + cols, s : s + 1] * key[s : s + 1]
        new_mem[0, s] = state
        read = jnp.where(lane == s, jnp.sum(state * query[s : s + 1], axis=1, keepdims=True), read)
    square = jnp.concatenate([read, jnp.zeros((LANES - cols, LANES), jnp.float32)], axis=0)
    readout = square.T[:SEQS] / divisor
    gate = pltpu.roll(rounded(total), LANES - 2 * SEG - cols, 1)
    gated = jax.nn.sigmoid(gate) * readout
    lanes = lax.broadcasted_iota(jnp.int32, gated.shape, 1)
    row = jnp.where(lanes < cols, gated, pltpu.roll(total, SEG, 1))
    if last:
        row = jnp.where(lanes < cols + SEG, row, pltpu.roll(first[...], 2 * SEG, 1))
    repeated(swap(row)[0], 4 if last else 2, sent)


def output_kernel(place, pieces, held, other, x, new_x, sent, wide):
    wide[...] = swap(pieces[...].astype(jnp.float32))
    update = contracted(place, wide, held, other, LANES, LANES + x.shape[1])
    total = (x[...].astype(jnp.float32) + update).astype(jnp.bfloat16)
    new_x[...] = total
    room = jnp.zeros((SEQS, LANES - x.shape[1]), jnp.float32)
    repeated(swap(jnp.concatenate([total.astype(jnp.float32), room], axis=1))[0], 2, sent)


def final_kernel(
    place, pieces, held, other, x, carried0, fresh0, carried1, fresh1, norm, max0, max1,
    new_x, new_norm, new_max, rows, gathered, wide,
):
    new_max[0] = max0[...]
    new_max[1] = max1[...]
    rows[...] = pieces[...].astype(jnp.float32)
    count = rows.shape[0] // 4
    for r in range(2):
        gathered[pl.ds(r, count, stride=2), :] = rows[pl.ds(r, count, stride=4), :]
    wide[...] = swap(gathered[...])
    low = LANES + x.shape[1]
    update = contracted(place, wide, held, other, low, low + x.shape[1])
    new_x[...] = (x[...].astype(jnp.float32) + update).astype(jnp.bfloat16)
    for layer, (carried, fresh) in enumerate(((carried0, fresh0), (carried1, fresh1))):
        keys = swap(rows[pl.ds(3 - layer, count, stride=4), :]) * DK ** (-0.5)
        for h in range(H):
            new_norm[layer, :, h, :] = (
                carried[:, h : h + 1] * norm[layer, :, h, :] + fresh[:, h : h + 1] * keys[(h + H // TURN) % H]
            )


SMEM = pl.BlockSpec(memory_space=pltpu.SMEM)
VMEM = pl.BlockSpec(memory_space=pltpu.VMEM)


def f32(*shape):
    return jax.ShapeDtypeStruct(shape, jnp.float32)


def bf16(*shape):
    return jax.ShapeDtypeStruct(shape, jnp.bfloat16)


def layer_block(shape, layer):
    return pl.BlockSpec((1, *shape[1:]), lambda i: (layer,) + (0,) * (len(shape) - 1))


def room(mib=12):
    return pltpu.CompilerParams(vmem_limit_bytes=mib << 20)


def cost(flops):
    return pl.CostEstimate(flops=flops, bytes_accessed=1 << 20, transcendentals=0)


def prepare(x, projections, w_output, devices):
    args = [x, *[w.transpose(0, 2, 1) for w in projections], w_output.transpose(0, 2, 1)]
    rows = args[1].shape[2]
    cols = sum(w.shape[0] * w.shape[1] for w in args[1:])
    return pl.pallas_call(
        prepare_kernel,
        out_shape=(bf16(2 * devices, LANES), bf16(cols, rows)),
        in_specs=[VMEM] + [pl.BlockSpec(memory_space=pltpu.HBM)] * (len(args) - 1),
        out_specs=[VMEM] * 2,
        scratch_shapes=[pltpu.SemaphoreType.DMA((2 * len(projections) + BLOCKS,))],
        compiler_params=room(60),
        cost_estimate=cost(1 << 23),
        name="prepare",
    )(*args)


def project(layer, place, pieces, gain, held, other, bias, max_state):
    tall = pieces.shape[0] // SEQS
    low = (LANES + 2 * DV // SEQS) * layer
    return pl.pallas_call(
        functools.partial(project_kernel, low=low),
        out_shape=(bf16(16, LANES), f32(SEQS, LANES), *[f32(SEQS, H)] * 3),
        in_specs=[SMEM] + [VMEM] * 6,
        out_specs=[VMEM] * 5,
        scratch_shapes=[pltpu.VMEM((tall, SEQS, LANES), jnp.float32)],
        compiler_params=room(),
        cost_estimate=cost(1 << 23),
        name="project",
    )(place, pieces, gain.reshape(tall, LANES), held, other, bias.reshape(1, H), max_state)


def renew(layer, place, pieces, product, first, carried, fresh, norm, mem, new_mem, devices):
    last = new_mem is not None
    args = [place, pieces, product] + ([first] if last else []) + [carried, fresh, norm, mem]
    whole = lambda a: pl.BlockSpec(a.shape, lambda i: (0,) * a.ndim)
    specs = [SMEM] + [whole(a) for a in args[1:-2]] + [layer_block(norm.shape, layer), layer_block(mem.shape, layer)]
    aliases = {}
    if last:
        aliases = {len(args): 0}
        args.append(new_mem)
        specs.append(pl.BlockSpec(memory_space=pl.ANY))
    rows = (4 if last else 2) * devices
    return pl.pallas_call(
        functools.partial(state_kernel, last=last),
        grid=(1,),
        out_shape=(f32(*mem.shape), bf16(rows, LANES)),
        in_specs=specs,
        out_specs=(layer_block(mem.shape, layer), pl.BlockSpec((rows, LANES), lambda i: (0, 0))),
        scratch_shapes=[pltpu.VMEM((2 * SEQS, LANES), jnp.float32)],
        input_output_aliases=aliases,
        compiler_params=room(),
        cost_estimate=cost(1 << 23),
        name="renew_last" if last else "renew",
    )(*args)


def output(place, pieces, held, other, x):
    return pl.pallas_call(
        output_kernel,
        out_shape=(bf16(*x.shape), bf16(*pieces.shape)),
        in_specs=[SMEM] + [VMEM] * 4,
        out_specs=[VMEM] * 2,
        scratch_shapes=[pltpu.VMEM((pieces.shape[0] // SEQS, SEQS, LANES), jnp.float32)],
        compiler_params=room(),
        cost_estimate=cost(1 << 23),
        name="output",
    )(place, pieces, held, other, x)


def final(place, pieces, held, other, x, gates, norm, maxima):
    half = pieces.shape[0] // 2
    return pl.pallas_call(
        final_kernel,
        out_shape=(bf16(*x.shape), f32(*norm.shape), f32(BLOCKS, SEQS, H)),
        in_specs=[SMEM] + [VMEM] * 11,
        out_specs=[VMEM] * 3,
        scratch_shapes=[
            pltpu.VMEM((2 * half, LANES), jnp.float32),
            pltpu.VMEM((half, LANES), jnp.float32),
            pltpu.VMEM((half // SEQS, SEQS, LANES), jnp.float32),
        ],
        compiler_params=room(),
        cost_estimate=cost(1 << 23),
        name="final",
    )(place, pieces, held, other, x, *gates[0], *gates[1], norm, *maxima)


def head_groups():
    size = lax.axis_size("t")
    return [list(range(at, at + PER_HEAD)) for at in range(0, size, PER_HEAD)]


def turned_group():
    size = lax.axis_size("t")
    return [[(i + size // TURN) % size for i in range(size)]]


def to_all(sent, groups):
    size = len(groups[0])
    got = lax.all_to_all(
        sent.reshape(size, -1, LANES), "t", 0, 0, axis_index_groups=groups, tiled=True
    )
    return got.reshape(-1, LANES)


def rows_to_all(w):
    size = lax.axis_size("x")
    got = [
        lax.ppermute(w, "x", [(i, (i + k) % size) for i in range(size)]) for k in range(1, size)
    ]
    held = jnp.stack([w, *got])
    other = lax.ppermute(held, "c", [(0, 1), (1, 0)])
    return held, other


def shards(
    tokens,
    norm_gain,
    w_query,
    w_key,
    w_value,
    w_outgate,
    w_ingate,
    w_forget,
    forget_bias,
    w_output,
    mem_state,
    norm_state,
    max_state,
):
    devices = lax.axis_size("t")
    spots = [lax.axis_index("x"), lax.axis_index("c"), lax.axis_index("t") // PER_HEAD]
    place = jnp.stack(spots).astype(jnp.int32)
    projections = (w_query, w_key, w_value, w_outgate, w_ingate, w_forget)

    sent, lines = prepare(tokens, projections, w_output, devices)
    weights = rows_to_all(lines)
    current = tokens
    gates, maxima, new_mem, first = ([], [], None, None)
    for layer in range(BLOCKS):
        pieces = to_all(sent, turned_group())
        sent, product, new_max, carried, fresh = project(
            layer, place, pieces, norm_gain[layer], *weights, forget_bias[layer], max_state[layer]
        )
        pieces = to_all(sent, head_groups())
        new_mem, sent = renew(
            layer, place, pieces, product, first, carried, fresh, norm_state, mem_state, new_mem, devices
        )
        first = product
        gates.append((carried, fresh))
        maxima.append(new_max)
        pieces = to_all(sent, turned_group())
        if layer < BLOCKS - 1:
            current, sent = output(place, pieces, *weights, current)
    current, new_norm, new_max = final(place, pieces, *weights, current, gates, norm_state, maxima)
    return (current, new_mem, new_norm, new_max)


def solution(mesh):
    dp = ("x", "c")
    split = Mesh(
        mesh.devices.reshape(mesh.shape["tp"], mesh.shape["dp"] // 2, 2), ("t", "x", "c")
    )

    return jax.shard_map(
        shards,
        mesh=split,
        in_specs=(
            P(dp, "t"),
            P(),
            P(None, dp, "t"),
            P(None, dp, "t"),
            P(None, dp, "t"),
            P(None, dp, "t"),
            P(None, dp, None),
            P(None, dp, None),
            P(),
            P(None, dp, "t"),
            P(None, dp, "t", None),
            P(None, dp, None, None),
            P(None, dp, None),
        ),
        out_specs=(
            P(dp, "t"),
            P(None, dp, "t", None),
            P(None, dp, None, None),
            P(None, dp, None),
        ),
        check_vma=False,
    )
```

```python
import functools

import jax
import jax.numpy as jnp
from jax import lax
from jax.experimental import pallas as pl
from jax.experimental.pallas import tpu as pltpu
from jax.sharding import Mesh
from jax.sharding import PartitionSpec as P


H = 16
DK = 128
DV = 256
BLOCKS = 2
EPSILON = 1e-06
LANES = 128
SEG = 16
SEQS = 8

PER_HEAD = 8
TURN = 2


def swap(x):
    x = x.reshape(-1, SEQS, LANES)
    row = lax.broadcasted_iota(jnp.int32, x.shape, 1)
    seg = lax.broadcasted_iota(jnp.int32, x.shape, 2) // SEG
    off = (seg - row + SEQS) % SEQS
    out = x
    for k in range(1, SEQS):
        moved = pltpu.roll(pltpu.roll(x, SEQS - k, 1), SEG * k, 2)
        out = jnp.where(off == k, moved, out)
    return out


def repeated(rows, count, ref):
    at = lax.broadcasted_iota(jnp.int32, rows.shape, 0) % count
    tile = jnp.broadcast_to(rows[0:1], rows.shape)
    for i in range(1, count):
        tile = jnp.where(at == i, jnp.broadcast_to(rows[i : i + 1], rows.shape), tile)
    tile = tile.astype(jnp.bfloat16)
    ref[...] = jnp.concatenate([tile] * (ref.shape[0] // SEQS), axis=0)


def rounded(x):
    return x.astype(jnp.bfloat16).astype(jnp.float32)


def contracted(wide, held, other, low, high):
    x, core = lax.axis_index("x"), lax.axis_index("c")
    slots = held.shape[0]
    per = held.shape[2] // LANES
    total = None
    for k in range(slots):
        chip = lax.rem(x - k + slots, slots) * 2
        for ref, block in ((held, chip + core), (other, chip + 1 - core)):
            block = lax.rem(block + slots, 2 * slots)
            part = wide[pl.ds(block * per, per)].astype(jnp.bfloat16)
            lhs = jnp.concatenate([part[i] for i in range(per)], axis=1)
            term = lax.dot_general(
                lhs, ref[k, low:high, :], (((1,), (1,)), ((), ())), preferred_element_type=jnp.float32
            )
            total = term if total is None else total + term
    return total


def prepare_kernel(*refs):
    x, sent, lines, sems = refs[0], refs[-3], refs[-2], refs[-1]
    weights, w_out = refs[1:-4], refs[-4]
    order = [(w, 0) for w in weights] + [(w_out, b) for b in range(BLOCKS)] + [(w, 1) for w in weights]
    copies, at = ([], 0)
    for i, (w, layer) in enumerate(order):
        copies.append(
            pltpu.make_async_copy(w.at[layer], lines.at[pl.ds(at, w.shape[1])], sems.at[i])
        )
        at += w.shape[1]
    for copy in copies:
        copy.start()
    room = jnp.zeros((SEQS, LANES - x.shape[1]), jnp.float32)
    repeated(swap(jnp.concatenate([x[...].astype(jnp.float32), room], axis=1))[0], 2, sent)
    for copy in copies:
        copy.wait()


def project_kernel(
    pieces, gain, held, other, bias, max_state, sent, product, new_max, carried, fresh, wide, *, low
):
    x = swap(pieces[...].astype(jnp.float32))
    count = x.shape[0]
    squares = jnp.sum(jnp.sum(x * x, axis=0), axis=1, keepdims=True)
    scale = lax.rsqrt(squares / (count * LANES) + EPSILON)
    turned = jnp.concatenate([gain[count // TURN :], gain[: count // TURN]], axis=0)
    wide[...] = x * scale[None] * turned[:, None, :]
    total = contracted(wide, held, other, low, low + LANES)
    product[...] = total
    repeated(swap(total)[0], 2, sent)
    in_pre = total[:, LANES - 2 * H : LANES - H]
    forget = total[:, LANES - H :] + bias[...]
    log_forget = jnp.minimum(forget, 0.0) - jnp.log1p(jnp.exp(-jnp.abs(forget)))
    kept = log_forget + max_state[...]
    top = jnp.maximum(kept, in_pre)
    new_max[...] = top
    carried[...] = jnp.exp(kept - top)
    fresh[...] = jnp.exp(in_pre - top)


def state_kernel(*refs, layer, last):
    if last:
        pieces, product, first, carried, fresh, norm, mem, new_mem, sent, rows = refs
    else:
        pieces, product, carried, fresh, norm, mem, new_mem, sent, rows = refs
    rows[...] = pieces[...].astype(jnp.float32)
    query = swap(rows[pl.ds(0, SEQS, stride=2), :])[0]
    key = swap(rows[pl.ds(1, SEQS, stride=2), :])[0] * DK ** (-0.5)
    head = lax.axis_index("t") // PER_HEAD
    mine = lax.broadcasted_iota(jnp.int32, (SEQS, H), 1) == head
    carry = jnp.sum(jnp.where(mine, carried[...], 0.0), axis=1, keepdims=True)
    new = jnp.sum(jnp.where(mine, fresh[...], 0.0), axis=1, keepdims=True)
    old = norm[layer]
    at = lax.broadcasted_iota(jnp.int32, old.shape, 1) == head
    norm_own = carry * jnp.sum(jnp.where(at, old, 0.0), axis=1) + new * key
    divisor = jnp.maximum(jnp.abs(jnp.sum(norm_own * query, axis=1, keepdims=True)), 1.0)
    total = product[...]
    added = (rounded(total) * new).T
    cols = mem.shape[2]
    lane = lax.broadcasted_iota(jnp.int32, (cols, LANES), 1)
    read = jnp.zeros((cols, LANES), jnp.float32)
    for s in range(SEQS):
        state = carry[s : s + 1] * mem[layer, s] + added[2 * SEG : 2 * SEG + cols, s : s + 1] * key[s : s + 1]
        new_mem[s] = state
        read = jnp.where(lane == s, jnp.sum(state * query[s : s + 1], axis=1, keepdims=True), read)
    square = jnp.concatenate([read, jnp.zeros((LANES - cols, LANES), jnp.float32)], axis=0)
    readout = square.T[:SEQS] / divisor
    gate = pltpu.roll(rounded(total), LANES - 2 * SEG - cols, 1)
    gated = jax.nn.sigmoid(gate) * readout
    lanes = lax.broadcasted_iota(jnp.int32, gated.shape, 1)
    row = jnp.where(lanes < cols, gated, pltpu.roll(total, SEG, 1))
    if last:
        row = jnp.where(lanes < cols + SEG, row, pltpu.roll(first[...], 2 * SEG, 1))
    repeated(swap(row)[0], 4 if last else 2, sent)


def output_kernel(pieces, held, other, x, new_x, sent, wide):
    wide[...] = swap(pieces[...].astype(jnp.float32))
    update = contracted(wide, held, other, LANES, LANES + x.shape[1])
    total = (x[...].astype(jnp.float32) + update).astype(jnp.bfloat16)
    new_x[...] = total
    room = jnp.zeros((SEQS, LANES - x.shape[1]), jnp.float32)
    repeated(swap(jnp.concatenate([total.astype(jnp.float32), room], axis=1))[0], 2, sent)


def final_kernel(
    pieces, held, other, x, carried0, fresh0, carried1, fresh1, norm, max0, max1, state0, state1,
    new_x, new_norm, new_max, new_mem, rows, gathered, wide, sems,
):
    copies = [
        pltpu.make_async_copy(state, new_mem.at[layer], sems.at[layer])
        for layer, state in enumerate((state0, state1))
    ]
    for copy in copies:
        copy.start()
    new_max[0] = max0[...]
    new_max[1] = max1[...]
    rows[...] = pieces[...].astype(jnp.float32)
    count = rows.shape[0] // 4
    for r in range(2):
        gathered[pl.ds(r, count, stride=2), :] = rows[pl.ds(r, count, stride=4), :]
    wide[...] = swap(gathered[...])
    low = LANES + x.shape[1]
    update = contracted(wide, held, other, low, low + x.shape[1])
    new_x[...] = (x[...].astype(jnp.float32) + update).astype(jnp.bfloat16)
    for layer, (carried, fresh) in enumerate(((carried0, fresh0), (carried1, fresh1))):
        keys = swap(rows[pl.ds(3 - layer, count, stride=4), :]) * DK ** (-0.5)
        for h in range(H):
            new_norm[layer, :, h, :] = (
                carried[:, h : h + 1] * norm[layer, :, h, :] + fresh[:, h : h + 1] * keys[(h + H // TURN) % H]
            )
    for copy in copies:
        copy.wait()


VMEM = pl.BlockSpec(memory_space=pltpu.VMEM)


def f32(*shape):
    return jax.ShapeDtypeStruct(shape, jnp.float32)


def bf16(*shape):
    return jax.ShapeDtypeStruct(shape, jnp.bfloat16)


def room(mib=12):
    return pltpu.CompilerParams(vmem_limit_bytes=mib << 20)


def cost(flops):
    return pl.CostEstimate(flops=flops, bytes_accessed=1 << 20, transcendentals=0)


def prepare(x, projections, w_output, devices):
    args = [x, *[w.transpose(0, 2, 1) for w in projections], w_output.transpose(0, 2, 1)]
    rows = args[1].shape[2]
    cols = sum(w.shape[0] * w.shape[1] for w in args[1:])
    return pl.pallas_call(
        prepare_kernel,
        out_shape=(bf16(2 * devices, LANES), bf16(cols, rows)),
        in_specs=[VMEM] + [pl.BlockSpec(memory_space=pltpu.HBM)] * (len(args) - 1),
        out_specs=[VMEM] * 2,
        scratch_shapes=[pltpu.SemaphoreType.DMA((2 * len(projections) + BLOCKS,))],
        compiler_params=room(60),
        cost_estimate=cost(1 << 23),
        name="prepare",
    )(*args)


def project(layer, pieces, gain, held, other, bias, max_state):
    tall = pieces.shape[0] // SEQS
    low = (LANES + 2 * DV // SEQS) * layer
    return pl.pallas_call(
        functools.partial(project_kernel, low=low),
        out_shape=(bf16(16, LANES), f32(SEQS, LANES), *[f32(SEQS, H)] * 3),
        in_specs=[VMEM] * 6,
        out_specs=[VMEM] * 5,
        scratch_shapes=[pltpu.VMEM((tall, SEQS, LANES), jnp.float32)],
        compiler_params=room(),
        cost_estimate=cost(1 << 23),
        name="project",
    )(pieces, gain.reshape(tall, LANES), held, other, bias.reshape(1, H), max_state)


def renew(layer, pieces, product, first, carried, fresh, norm, mem, devices):
    last = first is not None
    args = [pieces, product] + ([first] if last else []) + [carried, fresh, norm, mem]
    return pl.pallas_call(
        functools.partial(state_kernel, layer=layer, last=last),
        out_shape=(f32(*mem.shape[1:]), bf16((4 if last else 2) * devices, LANES)),
        in_specs=[VMEM] * len(args),
        out_specs=[VMEM] * 2,
        scratch_shapes=[pltpu.VMEM((2 * SEQS, LANES), jnp.float32)],
        compiler_params=room(),
        cost_estimate=cost(1 << 23),
        name="renew_last" if last else "renew",
    )(*args)


def output(pieces, held, other, x):
    return pl.pallas_call(
        output_kernel,
        out_shape=(bf16(*x.shape), bf16(*pieces.shape)),
        in_specs=[VMEM] * 4,
        out_specs=[VMEM] * 2,
        scratch_shapes=[pltpu.VMEM((pieces.shape[0] // SEQS, SEQS, LANES), jnp.float32)],
        compiler_params=room(),
        cost_estimate=cost(1 << 23),
        name="output",
    )(pieces, held, other, x)


def final(pieces, held, other, x, gates, norm, maxima, states):
    half = pieces.shape[0] // 2
    return pl.pallas_call(
        final_kernel,
        out_shape=(
            bf16(*x.shape), f32(*norm.shape), f32(BLOCKS, SEQS, H), f32(BLOCKS, *states[0].shape)
        ),
        in_specs=[VMEM] * 13,
        out_specs=[VMEM] * 3 + [pl.BlockSpec(memory_space=pltpu.HBM)],
        scratch_shapes=[
            pltpu.VMEM((2 * half, LANES), jnp.float32),
            pltpu.VMEM((half, LANES), jnp.float32),
            pltpu.VMEM((half // SEQS, SEQS, LANES), jnp.float32),
            pltpu.SemaphoreType.DMA((BLOCKS,)),
        ],
        compiler_params=room(),
        cost_estimate=cost(1 << 23),
        name="final",
    )(pieces, held, other, x, *gates[0], *gates[1], norm, *maxima, *states)


def head_groups():
    size = lax.axis_size("t")
    return [list(range(at, at + PER_HEAD)) for at in range(0, size, PER_HEAD)]


def turned_group():
    size = lax.axis_size("t")
    return [[(i + size // TURN) % size for i in range(size)]]


def to_all(sent, groups):
    size = len(groups[0])
    got = lax.all_to_all(
        sent.reshape(size, -1, LANES), "t", 0, 0, axis_index_groups=groups, tiled=True
    )
    return got.reshape(-1, LANES)


def rows_to_all(w):
    size = lax.axis_size("x")
    got = [
        lax.ppermute(w, "x", [(i, (i + k) % size) for i in range(size)]) for k in range(1, size)
    ]
    held = jnp.stack([w, *got])
    other = lax.ppermute(held, "c", [(0, 1), (1, 0)])
    return held, other


def shards(
    tokens,
    norm_gain,
    w_query,
    w_key,
    w_value,
    w_outgate,
    w_ingate,
    w_forget,
    forget_bias,
    w_output,
    mem_state,
    norm_state,
    max_state,
):
    devices = lax.axis_size("t")
    projections = (w_query, w_key, w_value, w_outgate, w_ingate, w_forget)

    sent, lines = prepare(tokens, projections, w_output, devices)
    weights = rows_to_all(lines)
    current = tokens
    gates, maxima, states, first = ([], [], [], None)
    for layer in range(BLOCKS):
        pieces = to_all(sent, turned_group())
        sent, product, new_max, carried, fresh = project(
            layer, pieces, norm_gain[layer], *weights, forget_bias[layer], max_state[layer]
        )
        pieces = to_all(sent, head_groups())
        state, sent = renew(
            layer, pieces, product, first, carried, fresh, norm_state, mem_state, devices
        )
        first = product
        states.append(state)
        gates.append((carried, fresh))
        maxima.append(new_max)
        pieces = to_all(sent, turned_group())
        if layer < BLOCKS - 1:
            current, sent = output(pieces, *weights, current)
    current, new_norm, new_max, new_mem = final(
        pieces, *weights, current, gates, norm_state, maxima, states
    )
    return (current, new_mem, new_norm, new_max)


def solution(mesh):
    dp = ("x", "c")
    split = Mesh(
        mesh.devices.reshape(mesh.shape["tp"], mesh.shape["dp"] // 2, 2), ("t", "x", "c")
    )

    return jax.shard_map(
        shards,
        mesh=split,
        in_specs=(
            P(dp, "t"),
            P(),
            P(None, dp, "t"),
            P(None, dp, "t"),
            P(None, dp, "t"),
            P(None, dp, "t"),
            P(None, dp, None),
            P(None, dp, None),
            P(),
            P(None, dp, "t"),
            P(None, dp, "t", None),
            P(None, dp, None, None),
            P(None, dp, None),
        ),
        out_specs=(
            P(dp, "t"),
            P(None, dp, "t", None),
            P(None, dp, None, None),
            P(None, dp, None),
        ),
        check_vma=False,
    )
```

```python
import functools

import jax
import jax.numpy as jnp
from jax import lax
from jax.experimental import pallas as pl
from jax.experimental.pallas import tpu as pltpu
from jax.sharding import Mesh
from jax.sharding import PartitionSpec as P


H = 16
DK = 128
DV = 256
BLOCKS = 2
EPSILON = 1e-06
LANES = 128
SEG = 16
SEQS = 8

PER_HEAD = 8
PLANE = 4
STEP = 5


def swap(x):
    x = x.reshape(-1, SEQS, LANES)
    row = lax.broadcasted_iota(jnp.int32, x.shape, 1)
    seg = lax.broadcasted_iota(jnp.int32, x.shape, 2) // SEG
    off = (seg - row + SEQS) % SEQS
    out = x
    for k in range(1, SEQS):
        moved = pltpu.roll(pltpu.roll(x, SEQS - k, 1), SEG * k, 2)
        out = jnp.where(off == k, moved, out)
    return out


def planes(count):
    return [(count // 2 + STEP * p) % count for p in range(count)]


def repeated(rows, count, ref):
    at = lax.broadcasted_iota(jnp.int32, rows.shape, 0) % count
    tile = jnp.broadcast_to(rows[0:1], rows.shape)
    for i in range(1, count):
        tile = jnp.where(at == i, jnp.broadcast_to(rows[i : i + 1], rows.shape), tile)
    tile = tile.astype(jnp.bfloat16)
    ref[...] = jnp.concatenate([tile] * (ref.shape[0] // SEQS), axis=0)


def rounded(x):
    return x.astype(jnp.bfloat16).astype(jnp.float32)


def in_place(x, wide):
    for p, plane in enumerate(planes(x.shape[0])):
        wide[plane] = x[p]


def contracted(wide, held, other, low, high):
    x, core = lax.axis_index("x"), lax.axis_index("c")
    slots = held.shape[0]
    per = held.shape[2] // LANES
    total = None
    for k in range(slots):
        chip = lax.rem(x - k + slots, slots) * 2
        for ref, block in ((held, chip + core), (other, chip + 1 - core)):
            part = wide[pl.ds(block * per, per)].astype(jnp.bfloat16)
            lhs = jnp.concatenate([part[i] for i in range(per)], axis=1)
            term = lax.dot_general(
                lhs, ref[k, low:high, :], (((1,), (1,)), ((), ())), preferred_element_type=jnp.float32
            )
            total = term if total is None else total + term
    return total


def prepare_kernel(*refs):
    x, sent, lines, sems = refs[0], refs[-3], refs[-2], refs[-1]
    weights, w_out = refs[1:-4], refs[-4]
    order = [(w, 0) for w in weights] + [(w_out, b) for b in range(BLOCKS)] + [(w, 1) for w in weights]
    copies, at = ([], 0)
    for i, (w, layer) in enumerate(order):
        copies.append(
            pltpu.make_async_copy(w.at[layer], lines.at[pl.ds(at, w.shape[1])], sems.at[i])
        )
        at += w.shape[1]
    for copy in copies:
        copy.start()
    room = jnp.zeros((SEQS, LANES - x.shape[1]), jnp.float32)
    repeated(swap(jnp.concatenate([x[...].astype(jnp.float32), room], axis=1))[0], 2, sent)
    for copy in copies:
        copy.wait()


def project_kernel(
    pieces, gain, held, other, bias, max_state, sent, product, new_max, carried, fresh, wide, *, low
):
    x = swap(pieces[...].astype(jnp.float32))
    count = x.shape[0]
    squares = jnp.sum(jnp.sum(x * x, axis=0), axis=1, keepdims=True)
    scale = lax.rsqrt(squares / (count * LANES) + EPSILON)
    for p, plane in enumerate(planes(count)):
        wide[plane] = x[p] * scale * gain[plane : plane + 1]
    total = contracted(wide, held, other, low, low + LANES)
    product[...] = total
    repeated(swap(total)[0], 2, sent)
    in_pre = total[:, LANES - 2 * H : LANES - H]
    forget = total[:, LANES - H :] + bias[...]
    log_forget = jnp.minimum(forget, 0.0) - jnp.log1p(jnp.exp(-jnp.abs(forget)))
    kept = log_forget + max_state[...]
    top = jnp.maximum(kept, in_pre)
    new_max[...] = top
    carried[...] = jnp.exp(kept - top)
    fresh[...] = jnp.exp(in_pre - top)


def state_kernel(*refs, layer, last):
    if last:
        pieces, product, first, carried, fresh, norm, mem, new_mem, sent, rows = refs
    else:
        pieces, product, carried, fresh, norm, mem, new_mem, sent, rows = refs
    rows[...] = pieces[...].astype(jnp.float32)
    query = swap(rows[pl.ds(0, SEQS, stride=2), :])[0]
    key = swap(rows[pl.ds(1, SEQS, stride=2), :])[0] * DK ** (-0.5)
    head = lax.axis_index("t") // PER_HEAD
    mine = lax.broadcasted_iota(jnp.int32, (SEQS, H), 1) == head
    carry = jnp.sum(jnp.where(mine, carried[...], 0.0), axis=1, keepdims=True)
    new = jnp.sum(jnp.where(mine, fresh[...], 0.0), axis=1, keepdims=True)
    old = norm[layer]
    at = lax.broadcasted_iota(jnp.int32, old.shape, 1) == head
    norm_own = carry * jnp.sum(jnp.where(at, old, 0.0), axis=1) + new * key
    divisor = jnp.maximum(jnp.abs(jnp.sum(norm_own * query, axis=1, keepdims=True)), 1.0)
    total = product[...]
    added = (rounded(total) * new).T
    cols = mem.shape[2]
    lane = lax.broadcasted_iota(jnp.int32, (cols, LANES), 1)
    read = jnp.zeros((cols, LANES), jnp.float32)
    for s in range(SEQS):
        state = carry[s : s + 1] * mem[layer, s] + added[2 * SEG : 2 * SEG + cols, s : s + 1] * key[s : s + 1]
        new_mem[s] = state
        read = jnp.where(lane == s, jnp.sum(state * query[s : s + 1], axis=1, keepdims=True), read)
    square = jnp.concatenate([read, jnp.zeros((LANES - cols, LANES), jnp.float32)], axis=0)
    readout = square.T[:SEQS] / divisor
    gate = pltpu.roll(rounded(total), LANES - 2 * SEG - cols, 1)
    gated = jax.nn.sigmoid(gate) * readout
    lanes = lax.broadcasted_iota(jnp.int32, gated.shape, 1)
    row = jnp.where(lanes < cols, gated, pltpu.roll(total, SEG, 1))
    if last:
        row = jnp.where(lanes < cols + SEG, row, pltpu.roll(first[...], 2 * SEG, 1))
    repeated(swap(row)[0], 4 if last else 2, sent)


def output_kernel(pieces, held, other, x, new_x, sent, wide):
    in_place(swap(pieces[...].astype(jnp.float32)), wide)
    update = contracted(wide, held, other, LANES, LANES + x.shape[1])
    total = (x[...].astype(jnp.float32) + update).astype(jnp.bfloat16)
    new_x[...] = total
    room = jnp.zeros((SEQS, LANES - x.shape[1]), jnp.float32)
    repeated(swap(jnp.concatenate([total.astype(jnp.float32), room], axis=1))[0], 2, sent)


def final_kernel(
    pieces, held, other, x, carried0, fresh0, carried1, fresh1, norm, max0, max1, state0, state1,
    new_x, new_norm, new_max, new_mem, rows, gathered, wide, sems,
):
    copies = [
        pltpu.make_async_copy(state, new_mem.at[layer], sems.at[layer])
        for layer, state in enumerate((state0, state1))
    ]
    for copy in copies:
        copy.start()
    new_max[0] = max0[...]
    new_max[1] = max1[...]
    rows[...] = pieces[...].astype(jnp.float32)
    count = rows.shape[0] // 4
    for r in range(2):
        gathered[pl.ds(r, count, stride=2), :] = rows[pl.ds(r, count, stride=4), :]
    in_place(swap(gathered[...]), wide)
    low = LANES + x.shape[1]
    update = contracted(wide, held, other, low, low + x.shape[1])
    new_x[...] = (x[...].astype(jnp.float32) + update).astype(jnp.bfloat16)
    for layer, (carried, fresh) in enumerate(((carried0, fresh0), (carried1, fresh1))):
        for p, plane in enumerate(planes(count // PLANE)):
            gathered[PLANE * plane : PLANE * (plane + 1), :] = rows[
                pl.ds(4 * PLANE * p + 3 - layer, PLANE, stride=4), :
            ]
        keys = swap(gathered[:count]) * DK ** (-0.5)
        for h in range(H):
            new_norm[layer, :, h, :] = (
                carried[:, h : h + 1] * norm[layer, :, h, :] + fresh[:, h : h + 1] * keys[h]
            )
    for copy in copies:
        copy.wait()


VMEM = pl.BlockSpec(memory_space=pltpu.VMEM)


def f32(*shape):
    return jax.ShapeDtypeStruct(shape, jnp.float32)


def bf16(*shape):
    return jax.ShapeDtypeStruct(shape, jnp.bfloat16)


def room(mib=12):
    return pltpu.CompilerParams(vmem_limit_bytes=mib << 20)


def cost(flops):
    return pl.CostEstimate(flops=flops, bytes_accessed=1 << 20, transcendentals=0)


def prepare(x, projections, w_output, devices):
    args = [x, *[w.transpose(0, 2, 1) for w in projections], w_output.transpose(0, 2, 1)]
    rows = args[1].shape[2]
    cols = sum(w.shape[0] * w.shape[1] for w in args[1:])
    return pl.pallas_call(
        prepare_kernel,
        out_shape=(bf16(2 * devices, LANES), bf16(cols, rows)),
        in_specs=[VMEM] + [pl.BlockSpec(memory_space=pltpu.HBM)] * (len(args) - 1),
        out_specs=[VMEM] * 2,
        scratch_shapes=[pltpu.SemaphoreType.DMA((2 * len(projections) + BLOCKS,))],
        compiler_params=room(60),
        cost_estimate=cost(1 << 23),
        name="prepare",
    )(*args)


def project(layer, pieces, gain, held, other, bias, max_state):
    tall = pieces.shape[0] // SEQS
    low = (LANES + 2 * DV // SEQS) * layer
    return pl.pallas_call(
        functools.partial(project_kernel, low=low),
        out_shape=(bf16(16, LANES), f32(SEQS, LANES), *[f32(SEQS, H)] * 3),
        in_specs=[VMEM] * 6,
        out_specs=[VMEM] * 5,
        scratch_shapes=[pltpu.VMEM((tall, SEQS, LANES), jnp.float32)],
        compiler_params=room(),
        cost_estimate=cost(1 << 23),
        name="project",
    )(pieces, gain.reshape(tall, LANES), held, other, bias.reshape(1, H), max_state)


def renew(layer, pieces, product, first, carried, fresh, norm, mem, devices):
    last = first is not None
    args = [pieces, product] + ([first] if last else []) + [carried, fresh, norm, mem]
    return pl.pallas_call(
        functools.partial(state_kernel, layer=layer, last=last),
        out_shape=(f32(*mem.shape[1:]), bf16((4 if last else 2) * devices, LANES)),
        in_specs=[VMEM] * len(args),
        out_specs=[VMEM] * 2,
        scratch_shapes=[pltpu.VMEM((2 * SEQS, LANES), jnp.float32)],
        compiler_params=room(),
        cost_estimate=cost(1 << 23),
        name="renew_last" if last else "renew",
    )(*args)


def output(pieces, held, other, x):
    return pl.pallas_call(
        output_kernel,
        out_shape=(bf16(*x.shape), bf16(*pieces.shape)),
        in_specs=[VMEM] * 4,
        out_specs=[VMEM] * 2,
        scratch_shapes=[pltpu.VMEM((pieces.shape[0] // SEQS, SEQS, LANES), jnp.float32)],
        compiler_params=room(),
        cost_estimate=cost(1 << 23),
        name="output",
    )(pieces, held, other, x)


def final(pieces, held, other, x, gates, norm, maxima, states):
    half = pieces.shape[0] // 2
    return pl.pallas_call(
        final_kernel,
        out_shape=(
            bf16(*x.shape), f32(*norm.shape), f32(BLOCKS, SEQS, H), f32(BLOCKS, *states[0].shape)
        ),
        in_specs=[VMEM] * 13,
        out_specs=[VMEM] * 3 + [pl.BlockSpec(memory_space=pltpu.HBM)],
        scratch_shapes=[
            pltpu.VMEM((2 * half, LANES), jnp.float32),
            pltpu.VMEM((half, LANES), jnp.float32),
            pltpu.VMEM((half // SEQS, SEQS, LANES), jnp.float32),
            pltpu.SemaphoreType.DMA((BLOCKS,)),
        ],
        compiler_params=room(),
        cost_estimate=cost(1 << 23),
        name="final",
    )(pieces, held, other, x, *gates[0], *gates[1], norm, *maxima, *states)


def head_groups():
    size = lax.axis_size("t")
    return [list(range(at, at + PER_HEAD)) for at in range(0, size, PER_HEAD)]


def wide_group():
    order = planes(lax.axis_size("t") // PLANE)
    return [[plane * PLANE + i for plane in order for i in range(PLANE)]]


def to_all(sent, groups):
    size = len(groups[0])
    got = lax.all_to_all(
        sent.reshape(size, -1, LANES), "t", 0, 0, axis_index_groups=groups, tiled=True
    )
    return got.reshape(-1, LANES)


def rows_to_all(w):
    size = lax.axis_size("x")
    got = [lax.ppermute(w, "x", [(i, (i + k) % size) for i in range(size)]) for k in range(1, size)]
    held = jnp.stack([w, *got])
    other = lax.ppermute(held, "c", [(0, 1), (1, 0)])
    return held, other


def shards(
    tokens,
    norm_gain,
    w_query,
    w_key,
    w_value,
    w_outgate,
    w_ingate,
    w_forget,
    forget_bias,
    w_output,
    mem_state,
    norm_state,
    max_state,
):
    devices = lax.axis_size("t")
    projections = (w_query, w_key, w_value, w_outgate, w_ingate, w_forget)

    sent, lines = prepare(tokens, projections, w_output, devices)
    weights = rows_to_all(lines)
    current = tokens
    gates, maxima, states, first = ([], [], [], None)
    for layer in range(BLOCKS):
        pieces = to_all(sent, wide_group())
        sent, product, new_max, carried, fresh = project(
            layer, pieces, norm_gain[layer], *weights, forget_bias[layer], max_state[layer]
        )
        pieces = to_all(sent, head_groups())
        state, sent = renew(
            layer, pieces, product, first, carried, fresh, norm_state, mem_state, devices
        )
        first = product
        states.append(state)
        gates.append((carried, fresh))
        maxima.append(new_max)
        pieces = to_all(sent, wide_group())
        if layer < BLOCKS - 1:
            current, sent = output(pieces, *weights, current)
    current, new_norm, new_max, new_mem = final(
        pieces, *weights, current, gates, norm_state, maxima, states
    )
    return (current, new_mem, new_norm, new_max)


def solution(mesh):
    dp = ("x", "c")
    split = Mesh(
        mesh.devices.reshape(mesh.shape["tp"], mesh.shape["dp"] // 2, 2), ("t", "x", "c")
    )

    return jax.shard_map(
        shards,
        mesh=split,
        in_specs=(
            P(dp, "t"),
            P(),
            P(None, dp, "t"),
            P(None, dp, "t"),
            P(None, dp, "t"),
            P(None, dp, "t"),
            P(None, dp, None),
            P(None, dp, None),
            P(),
            P(None, dp, "t"),
            P(None, dp, "t", None),
            P(None, dp, None, None),
            P(None, dp, None),
        ),
        out_specs=(
            P(dp, "t"),
            P(None, dp, "t", None),
            P(None, dp, None, None),
            P(None, dp, None),
        ),
        check_vma=False,
    )
```

```python
import functools

import jax
import jax.numpy as jnp
from jax import lax
from jax.experimental import pallas as pl
from jax.experimental.pallas import tpu as pltpu
from jax.sharding import Mesh
from jax.sharding import PartitionSpec as P


H = 16
DK = 128
DV = 256
BLOCKS = 2
EPSILON = 1e-06
LANES = 128
SEG = 16
SEQS = 8

PER_HEAD = 8
BLOCK = 4
TURN = 5


def swap(x):
    x = x.reshape(-1, SEQS, LANES)
    row = lax.broadcasted_iota(jnp.int32, x.shape, 1)
    seg = lax.broadcasted_iota(jnp.int32, x.shape, 2) // SEG
    off = (seg - row + SEQS) % SEQS
    out = x
    for k in range(1, SEQS):
        moved = pltpu.roll(pltpu.roll(x, SEQS - k, 1), SEG * k, 2)
        out = jnp.where(off == k, moved, out)
    return out


def repeated(rows, count, ref):
    at = lax.broadcasted_iota(jnp.int32, rows.shape, 0) % count
    tile = jnp.broadcast_to(rows[0:1], rows.shape)
    for i in range(1, count):
        tile = jnp.where(at == i, jnp.broadcast_to(rows[i : i + 1], rows.shape), tile)
    tile = tile.astype(jnp.bfloat16)
    ref[...] = jnp.concatenate([tile] * (ref.shape[0] // SEQS), axis=0)


def rounded(x):
    return x.astype(jnp.bfloat16).astype(jnp.float32)


def contracted(wide, held, other, low, high):
    x, core = lax.axis_index("x"), lax.axis_index("c")
    slots = held.shape[0]
    per = held.shape[2] // LANES
    total = None
    for k in range(slots):
        chip = lax.rem(x - k + slots, slots) * 2
        for ref, block in ((held, chip + core), (other, chip + 1 - core)):
            block = lax.rem(block + 2 * slots - TURN, 2 * slots)
            part = wide[pl.ds(block * per, per)].astype(jnp.bfloat16)
            lhs = jnp.concatenate([part[i] for i in range(per)], axis=1)
            term = lax.dot_general(
                lhs, ref[k, low:high, :], (((1,), (1,)), ((), ())), preferred_element_type=jnp.float32
            )
            total = term if total is None else total + term
    return total


def prepare_kernel(*refs):
    x, sent, lines, sems = refs[0], refs[-3], refs[-2], refs[-1]
    weights, w_out = refs[1:-4], refs[-4]
    order = [(w, 0) for w in weights] + [(w_out, b) for b in range(BLOCKS)] + [(w, 1) for w in weights]
    copies, at = ([], 0)
    for i, (w, layer) in enumerate(order):
        copies.append(
            pltpu.make_async_copy(w.at[layer], lines.at[pl.ds(at, w.shape[1])], sems.at[i])
        )
        at += w.shape[1]
    for copy in copies:
        copy.start()
    room = jnp.zeros((SEQS, LANES - x.shape[1]), jnp.float32)
    repeated(swap(jnp.concatenate([x[...].astype(jnp.float32), room], axis=1))[0], 2, sent)
    for copy in copies:
        copy.wait()


def project_kernel(
    pieces, gain, held, other, bias, max_state, sent, product, new_max, carried, fresh, wide, *, low
):
    x = swap(pieces[...].astype(jnp.float32))
    count = x.shape[0]
    squares = jnp.sum(jnp.sum(x * x, axis=0), axis=1, keepdims=True)
    scale = lax.rsqrt(squares / (count * LANES) + EPSILON)
    turned = jnp.concatenate([gain[TURN * BLOCK :], gain[: TURN * BLOCK]], axis=0)
    wide[...] = x * scale[None] * turned[:, None, :]
    total = contracted(wide, held, other, low, low + LANES)
    product[...] = total
    repeated(swap(total)[0], 2, sent)
    in_pre = total[:, LANES - 2 * H : LANES - H]
    forget = total[:, LANES - H :] + bias[...]
    log_forget = jnp.minimum(forget, 0.0) - jnp.log1p(jnp.exp(-jnp.abs(forget)))
    kept = log_forget + max_state[...]
    top = jnp.maximum(kept, in_pre)
    new_max[...] = top
    carried[...] = jnp.exp(kept - top)
    fresh[...] = jnp.exp(in_pre - top)


def state_kernel(*refs, layer, last):
    if last:
        pieces, product, first, carried, fresh, norm, mem, new_mem, sent, rows = refs
    else:
        pieces, product, carried, fresh, norm, mem, new_mem, sent, rows = refs
    rows[...] = pieces[...].astype(jnp.float32)
    query = swap(rows[pl.ds(0, SEQS, stride=2), :])[0]
    key = swap(rows[pl.ds(1, SEQS, stride=2), :])[0] * DK ** (-0.5)
    head = lax.axis_index("t") // PER_HEAD
    mine = lax.broadcasted_iota(jnp.int32, (SEQS, H), 1) == head
    carry = jnp.sum(jnp.where(mine, carried[...], 0.0), axis=1, keepdims=True)
    new = jnp.sum(jnp.where(mine, fresh[...], 0.0), axis=1, keepdims=True)
    old = norm[layer]
    at = lax.broadcasted_iota(jnp.int32, old.shape, 1) == head
    norm_own = carry * jnp.sum(jnp.where(at, old, 0.0), axis=1) + new * key
    divisor = jnp.maximum(jnp.abs(jnp.sum(norm_own * query, axis=1, keepdims=True)), 1.0)
    total = product[...]
    added = (rounded(total) * new).T
    cols = mem.shape[2]
    lane = lax.broadcasted_iota(jnp.int32, (cols, LANES), 1)
    read = jnp.zeros((cols, LANES), jnp.float32)
    for s in range(SEQS):
        state = carry[s : s + 1] * mem[layer, s] + added[2 * SEG : 2 * SEG + cols, s : s + 1] * key[s : s + 1]
        new_mem[s] = state
        read = jnp.where(lane == s, jnp.sum(state * query[s : s + 1], axis=1, keepdims=True), read)
    square = jnp.concatenate([read, jnp.zeros((LANES - cols, LANES), jnp.float32)], axis=0)
    readout = square.T[:SEQS] / divisor
    gate = pltpu.roll(rounded(total), LANES - 2 * SEG - cols, 1)
    gated = jax.nn.sigmoid(gate) * readout
    lanes = lax.broadcasted_iota(jnp.int32, gated.shape, 1)
    row = jnp.where(lanes < cols, gated, pltpu.roll(total, SEG, 1))
    if last:
        row = jnp.where(lanes < cols + SEG, row, pltpu.roll(first[...], 2 * SEG, 1))
    repeated(swap(row)[0], 4 if last else 2, sent)


def output_kernel(pieces, held, other, x, new_x, sent, wide):
    wide[...] = swap(pieces[...].astype(jnp.float32))
    update = contracted(wide, held, other, LANES, LANES + x.shape[1])
    total = (x[...].astype(jnp.float32) + update).astype(jnp.bfloat16)
    new_x[...] = total
    room = jnp.zeros((SEQS, LANES - x.shape[1]), jnp.float32)
    repeated(swap(jnp.concatenate([total.astype(jnp.float32), room], axis=1))[0], 2, sent)


def final_kernel(
    pieces, held, other, x, carried0, fresh0, carried1, fresh1, norm, max0, max1, state0, state1,
    new_x, new_max, new_norm, new_mem, rows, gathered, wide, norm_now, sems,
):
    copies = [
        pltpu.make_async_copy(state, new_mem.at[layer], sems.at[layer])
        for layer, state in enumerate((state0, state1))
    ]
    for copy in copies:
        copy.start()
    new_max[0] = max0[...]
    new_max[1] = max1[...]
    rows[...] = pieces[...].astype(jnp.float32)
    count = rows.shape[0] // 4
    for layer, (carried, fresh) in enumerate(((carried0, fresh0), (carried1, fresh1))):
        keys = swap(rows[pl.ds(3 - layer, count, stride=4), :]) * DK ** (-0.5)
        for h in range(H):
            norm_now[layer, :, h, :] = (
                carried[:, h : h + 1] * norm[layer, :, h, :]
                + fresh[:, h : h + 1] * keys[(h - 2 * TURN) % H]
            )
        copies.append(
            pltpu.make_async_copy(norm_now.at[layer], new_norm.at[layer], sems.at[BLOCKS + layer])
        )
        copies[-1].start()
    for r in range(2):
        gathered[pl.ds(r, count, stride=2), :] = rows[pl.ds(r, count, stride=4), :]
    wide[...] = swap(gathered[...])
    low = LANES + x.shape[1]
    update = contracted(wide, held, other, low, low + x.shape[1])
    new_x[...] = (x[...].astype(jnp.float32) + update).astype(jnp.bfloat16)
    for copy in copies:
        copy.wait()


VMEM = pl.BlockSpec(memory_space=pltpu.VMEM)


def f32(*shape):
    return jax.ShapeDtypeStruct(shape, jnp.float32)


def bf16(*shape):
    return jax.ShapeDtypeStruct(shape, jnp.bfloat16)


def room(mib=12):
    return pltpu.CompilerParams(vmem_limit_bytes=mib << 20)


def cost(flops):
    return pl.CostEstimate(flops=flops, bytes_accessed=1 << 20, transcendentals=0)


def prepare(x, projections, w_output, devices):
    args = [x, *[w.transpose(0, 2, 1) for w in projections], w_output.transpose(0, 2, 1)]
    rows = args[1].shape[2]
    cols = sum(w.shape[0] * w.shape[1] for w in args[1:])
    return pl.pallas_call(
        prepare_kernel,
        out_shape=(bf16(2 * devices, LANES), bf16(cols, rows)),
        in_specs=[VMEM] + [pl.BlockSpec(memory_space=pltpu.HBM)] * (len(args) - 1),
        out_specs=[VMEM] * 2,
        scratch_shapes=[pltpu.SemaphoreType.DMA((2 * len(projections) + BLOCKS,))],
        compiler_params=room(60),
        cost_estimate=cost(1 << 23),
        name="prepare",
    )(*args)


def project(layer, pieces, gain, held, other, bias, max_state):
    tall = pieces.shape[0] // SEQS
    low = (LANES + 2 * DV // SEQS) * layer
    return pl.pallas_call(
        functools.partial(project_kernel, low=low),
        out_shape=(bf16(16, LANES), f32(SEQS, LANES), *[f32(SEQS, H)] * 3),
        in_specs=[VMEM] * 6,
        out_specs=[VMEM] * 5,
        scratch_shapes=[pltpu.VMEM((tall, SEQS, LANES), jnp.float32)],
        compiler_params=room(),
        cost_estimate=cost(1 << 23),
        name="project",
    )(pieces, gain.reshape(tall, LANES), held, other, bias.reshape(1, H), max_state)


def renew(layer, pieces, product, first, carried, fresh, norm, mem, devices):
    last = first is not None
    args = [pieces, product] + ([first] if last else []) + [carried, fresh, norm, mem]
    return pl.pallas_call(
        functools.partial(state_kernel, layer=layer, last=last),
        out_shape=(f32(*mem.shape[1:]), bf16((4 if last else 2) * devices, LANES)),
        in_specs=[VMEM] * len(args),
        out_specs=[VMEM] * 2,
        scratch_shapes=[pltpu.VMEM((2 * SEQS, LANES), jnp.float32)],
        compiler_params=room(),
        cost_estimate=cost(1 << 23),
        name="renew_last" if last else "renew",
    )(*args)


def output(pieces, held, other, x):
    return pl.pallas_call(
        output_kernel,
        out_shape=(bf16(*x.shape), bf16(*pieces.shape)),
        in_specs=[VMEM] * 4,
        out_specs=[VMEM] * 2,
        scratch_shapes=[pltpu.VMEM((pieces.shape[0] // SEQS, SEQS, LANES), jnp.float32)],
        compiler_params=room(),
        cost_estimate=cost(1 << 23),
        name="output",
    )(pieces, held, other, x)


def final(pieces, held, other, x, gates, norm, maxima, states):
    half = pieces.shape[0] // 2
    return pl.pallas_call(
        final_kernel,
        out_shape=(
            bf16(*x.shape), f32(BLOCKS, SEQS, H), f32(*norm.shape), f32(BLOCKS, *states[0].shape)
        ),
        in_specs=[VMEM] * 13,
        out_specs=[VMEM] * 2 + [pl.BlockSpec(memory_space=pltpu.HBM)] * 2,
        scratch_shapes=[
            pltpu.VMEM((2 * half, LANES), jnp.float32),
            pltpu.VMEM((half, LANES), jnp.float32),
            pltpu.VMEM((half // SEQS, SEQS, LANES), jnp.float32),
            pltpu.VMEM(norm.shape, jnp.float32),
            pltpu.SemaphoreType.DMA((2 * BLOCKS,)),
        ],
        compiler_params=room(),
        cost_estimate=cost(1 << 23),
        name="final",
    )(pieces, held, other, x, *gates[0], *gates[1], norm, *maxima, *states)


def head_groups():
    size = lax.axis_size("t")
    return [list(range(at, at + PER_HEAD)) for at in range(0, size, PER_HEAD)]


def turned_group():
    size = lax.axis_size("t")
    return [[(i + TURN * BLOCK * 4) % size for i in range(size)]]


def to_all(sent, groups):
    size = len(groups[0])
    got = lax.all_to_all(
        sent.reshape(size, -1, LANES), "t", 0, 0, axis_index_groups=groups, tiled=True
    )
    return got.reshape(-1, LANES)


def rows_to_all(w):
    size = lax.axis_size("x")
    got = [lax.ppermute(w, "x", [(i, (i + k) % size) for i in range(size)]) for k in range(1, size)]
    held = jnp.stack([w, *got])
    other = lax.ppermute(held, "c", [(0, 1), (1, 0)])
    return held, other


def shards(
    tokens,
    norm_gain,
    w_query,
    w_key,
    w_value,
    w_outgate,
    w_ingate,
    w_forget,
    forget_bias,
    w_output,
    mem_state,
    norm_state,
    max_state,
):
    devices = lax.axis_size("t")
    projections = (w_query, w_key, w_value, w_outgate, w_ingate, w_forget)

    sent, lines = prepare(tokens, projections, w_output, devices)
    weights = rows_to_all(lines)
    current = tokens
    gates, maxima, states, first = ([], [], [], None)
    for layer in range(BLOCKS):
        pieces = to_all(sent, turned_group())
        sent, product, new_max, carried, fresh = project(
            layer, pieces, norm_gain[layer], *weights, forget_bias[layer], max_state[layer]
        )
        pieces = to_all(sent, head_groups())
        state, sent = renew(
            layer, pieces, product, first, carried, fresh, norm_state, mem_state, devices
        )
        first = product
        states.append(state)
        gates.append((carried, fresh))
        maxima.append(new_max)
        pieces = to_all(sent, turned_group())
        if layer < BLOCKS - 1:
            current, sent = output(pieces, *weights, current)
    current, new_max, new_norm, new_mem = final(
        pieces, *weights, current, gates, norm_state, maxima, states
    )
    return (current, new_mem, new_norm, new_max)


def solution(mesh):
    dp = ("x", "c")
    split = Mesh(
        mesh.devices.reshape(mesh.shape["tp"], mesh.shape["dp"] // 2, 2), ("t", "x", "c")
    )

    return jax.shard_map(
        shards,
        mesh=split,
        in_specs=(
            P(dp, "t"),
            P(),
            P(None, dp, "t"),
            P(None, dp, "t"),
            P(None, dp, "t"),
            P(None, dp, "t"),
            P(None, dp, None),
            P(None, dp, None),
            P(),
            P(None, dp, "t"),
            P(None, dp, "t", None),
            P(None, dp, None, None),
            P(None, dp, None),
        ),
        out_specs=(
            P(dp, "t"),
            P(None, dp, "t", None),
            P(None, dp, None, None),
            P(None, dp, None),
        ),
        check_vma=False,
    )
```

```python
import functools

import jax
import jax.numpy as jnp
from jax import lax
from jax.experimental import pallas as pl
from jax.experimental.pallas import tpu as pltpu
from jax.sharding import Mesh
from jax.sharding import PartitionSpec as P


H = 16
DK = 128
DV = 256
BLOCKS = 2
EPSILON = 1e-06
LANES = 128
SEG = 16
SEQS = 8

PER_HEAD = 8
TURN = 2


def swap(x):
    x = x.reshape(-1, SEQS, LANES)
    row = lax.broadcasted_iota(jnp.int32, x.shape, 1)
    seg = lax.broadcasted_iota(jnp.int32, x.shape, 2) // SEG
    off = (seg - row + SEQS) % SEQS
    out = x
    for k in range(1, SEQS):
        moved = pltpu.roll(pltpu.roll(x, SEQS - k, 1), SEG * k, 2)
        out = jnp.where(off == k, moved, out)
    return out


def repeated(rows, count, ref):
    at = lax.broadcasted_iota(jnp.int32, rows.shape, 0) % count
    tile = jnp.broadcast_to(rows[0:1], rows.shape)
    for i in range(1, count):
        tile = jnp.where(at == i, jnp.broadcast_to(rows[i : i + 1], rows.shape), tile)
    tile = tile.astype(jnp.bfloat16)
    ref[...] = jnp.concatenate([tile] * (ref.shape[0] // SEQS), axis=0)


def rounded(x):
    return x.astype(jnp.bfloat16).astype(jnp.float32)


def contracted(wide, held, other, low, high):
    x, core = lax.axis_index("x"), lax.axis_index("c")
    slots = held.shape[0]
    per = held.shape[2] // LANES
    total = None
    for k in range(slots):
        chip = lax.rem(x - k + slots, slots) * 2
        for ref, block in ((held, chip + core), (other, chip + 1 - core)):
            block = lax.rem(block + slots, 2 * slots)
            part = wide[pl.ds(block * per, per)].astype(jnp.bfloat16)
            lhs = jnp.concatenate([part[i] for i in range(per)], axis=1)
            term = lax.dot_general(
                lhs, ref[k, low:high, :], (((1,), (1,)), ((), ())), preferred_element_type=jnp.float32
            )
            total = term if total is None else total + term
    return total


def prepare_kernel(*refs):
    x, sent, lines, message, packed, sems = refs[0], *refs[-5:]
    weights, w_out = refs[1:-6], refs[-6]
    order = [(w, 0) for w in weights] + [(w_out, b) for b in range(BLOCKS)] + [(w, 1) for w in weights]
    copies, at = ([], 0)
    for i, (w, layer) in enumerate(order):
        copies.append(
            pltpu.make_async_copy(w.at[layer], packed.at[pl.ds(at, w.shape[1])], sems.at[i])
        )
        at += w.shape[1]
    for copy in copies:
        copy.start()
    room = jnp.zeros((SEQS, LANES - x.shape[1]), jnp.float32)
    repeated(swap(jnp.concatenate([x[...].astype(jnp.float32), room], axis=1))[0], 2, message)
    out = [
        pltpu.make_async_copy(message, sent, sems.at[len(copies)]),
        pltpu.make_async_copy(packed, lines, sems.at[len(copies) + 1]),
    ]
    out[0].start()
    for copy in copies:
        copy.wait()
    out[1].start()
    for copy in out:
        copy.wait()


def project_kernel(
    pieces, gain, held, other, bias, max_state, sent, product, new_max, carried, fresh, wide, *, low
):
    x = swap(pieces[...].astype(jnp.float32))
    count = x.shape[0]
    squares = jnp.sum(jnp.sum(x * x, axis=0), axis=1, keepdims=True)
    scale = lax.rsqrt(squares / (count * LANES) + EPSILON)
    turned = jnp.concatenate([gain[count // TURN :], gain[: count // TURN]], axis=0)
    wide[...] = x * scale[None] * turned[:, None, :]
    total = contracted(wide, held, other, low, low + LANES)
    product[...] = total
    repeated(swap(total)[0], 2, sent)
    in_pre = total[:, LANES - 2 * H : LANES - H]
    forget = total[:, LANES - H :] + bias[...]
    log_forget = jnp.minimum(forget, 0.0) - jnp.log1p(jnp.exp(-jnp.abs(forget)))
    kept = log_forget + max_state[...]
    top = jnp.maximum(kept, in_pre)
    new_max[...] = top
    carried[...] = jnp.exp(kept - top)
    fresh[...] = jnp.exp(in_pre - top)


def state_kernel(*refs, layer, last):
    if last:
        pieces, product, first, carried, fresh, norm, mem, new_mem, sent, rows = refs
    else:
        pieces, product, carried, fresh, norm, mem, new_mem, sent, rows = refs
    rows[...] = pieces[...].astype(jnp.float32)
    query = swap(rows[pl.ds(0, SEQS, stride=2), :])[0]
    key = swap(rows[pl.ds(1, SEQS, stride=2), :])[0] * DK ** (-0.5)
    head = lax.axis_index("t") // PER_HEAD
    mine = lax.broadcasted_iota(jnp.int32, (SEQS, H), 1) == head
    carry = jnp.sum(jnp.where(mine, carried[...], 0.0), axis=1, keepdims=True)
    new = jnp.sum(jnp.where(mine, fresh[...], 0.0), axis=1, keepdims=True)
    old = norm[layer]
    at = lax.broadcasted_iota(jnp.int32, old.shape, 1) == head
    norm_own = carry * jnp.sum(jnp.where(at, old, 0.0), axis=1) + new * key
    divisor = jnp.maximum(jnp.abs(jnp.sum(norm_own * query, axis=1, keepdims=True)), 1.0)
    total = product[...]
    added = (rounded(total) * new).T
    cols = mem.shape[2]
    lane = lax.broadcasted_iota(jnp.int32, (cols, LANES), 1)
    read = jnp.zeros((cols, LANES), jnp.float32)
    for s in range(SEQS):
        state = carry[s : s + 1] * mem[layer, s] + added[2 * SEG : 2 * SEG + cols, s : s + 1] * key[s : s + 1]
        new_mem[s] = state
        read = jnp.where(lane == s, jnp.sum(state * query[s : s + 1], axis=1, keepdims=True), read)
    square = jnp.concatenate([read, jnp.zeros((LANES - cols, LANES), jnp.float32)], axis=0)
    readout = square.T[:SEQS] / divisor
    gate = pltpu.roll(rounded(total), LANES - 2 * SEG - cols, 1)
    gated = jax.nn.sigmoid(gate) * readout
    lanes = lax.broadcasted_iota(jnp.int32, gated.shape, 1)
    row = jnp.where(lanes < cols, gated, pltpu.roll(total, SEG, 1))
    if last:
        row = jnp.where(lanes < cols + SEG, row, pltpu.roll(first[...], 2 * SEG, 1))
    repeated(swap(row)[0], 4 if last else 2, sent)


def output_kernel(pieces, held, other, x, new_x, sent, wide):
    wide[...] = swap(pieces[...].astype(jnp.float32))
    update = contracted(wide, held, other, LANES, LANES + x.shape[1])
    total = (x[...].astype(jnp.float32) + update).astype(jnp.bfloat16)
    new_x[...] = total
    room = jnp.zeros((SEQS, LANES - x.shape[1]), jnp.float32)
    repeated(swap(jnp.concatenate([total.astype(jnp.float32), room], axis=1))[0], 2, sent)


def final_kernel(
    pieces, held, other, x, carried0, fresh0, carried1, fresh1, norm, max0, max1, state0, state1,
    new_x, new_norm, new_max, new_mem, rows, gathered, wide, x_now, norm_now, sems,
):
    copies = [
        pltpu.make_async_copy(src, dst.at[layer], sems.at[i, layer])
        for i, (pair, dst) in enumerate((((state0, state1), new_mem), ((max0, max1), new_max)))
        for layer, src in enumerate(pair)
    ]
    for copy in copies:
        copy.start()
    rows[...] = pieces[...].astype(jnp.float32)
    count = rows.shape[0] // 4
    for r in range(2):
        gathered[pl.ds(r, count, stride=2), :] = rows[pl.ds(r, count, stride=4), :]
    wide[...] = swap(gathered[...])
    low = LANES + x.shape[1]
    update = contracted(wide, held, other, low, low + x.shape[1])
    x_now[...] = (x[...].astype(jnp.float32) + update).astype(jnp.bfloat16)
    for layer, (carried, fresh) in enumerate(((carried0, fresh0), (carried1, fresh1))):
        keys = swap(rows[pl.ds(3 - layer, count, stride=4), :]) * DK ** (-0.5)
        for h in range(H):
            norm_now[layer, :, h, :] = (
                carried[:, h : h + 1] * norm[layer, :, h, :]
                + fresh[:, h : h + 1] * keys[(h + H // TURN) % H]
            )
    late = [
        pltpu.make_async_copy(x_now, new_x, sems.at[2, 0]),
        pltpu.make_async_copy(norm_now, new_norm, sems.at[2, 1]),
    ]
    for copy in late:
        copy.start()
    for copy in copies + late:
        copy.wait()


VMEM = pl.BlockSpec(memory_space=pltpu.VMEM)
HBM = pl.BlockSpec(memory_space=pltpu.HBM)


def f32(*shape):
    return jax.ShapeDtypeStruct(shape, jnp.float32)


def bf16(*shape):
    return jax.ShapeDtypeStruct(shape, jnp.bfloat16)


def room(mib=12):
    return pltpu.CompilerParams(vmem_limit_bytes=mib << 20)


def cost(flops):
    return pl.CostEstimate(flops=flops, bytes_accessed=1 << 20, transcendentals=0)


def prepare(x, projections, w_output, devices):
    args = [x, *[w.transpose(0, 2, 1) for w in projections], w_output.transpose(0, 2, 1)]
    rows = args[1].shape[2]
    cols = sum(w.shape[0] * w.shape[1] for w in args[1:])
    return pl.pallas_call(
        prepare_kernel,
        out_shape=(bf16(2 * devices, LANES), bf16(cols, rows)),
        in_specs=[VMEM] + [HBM] * (len(args) - 1),
        out_specs=[HBM] * 2,
        scratch_shapes=[
            pltpu.VMEM((2 * devices, LANES), jnp.bfloat16),
            pltpu.VMEM((cols, rows), jnp.bfloat16),
            pltpu.SemaphoreType.DMA((2 * len(projections) + BLOCKS + 2,)),
        ],
        compiler_params=room(60),
        cost_estimate=cost(1 << 23),
        name="prepare",
    )(*args)


def project(layer, pieces, gain, held, other, bias, max_state):
    tall = pieces.shape[0] // SEQS
    low = (LANES + 2 * DV // SEQS) * layer
    return pl.pallas_call(
        functools.partial(project_kernel, low=low),
        out_shape=(bf16(16, LANES), f32(SEQS, LANES), *[f32(SEQS, H)] * 3),
        in_specs=[VMEM] * 6,
        out_specs=[VMEM] * 5,
        scratch_shapes=[pltpu.VMEM((tall, SEQS, LANES), jnp.float32)],
        compiler_params=room(),
        cost_estimate=cost(1 << 23),
        name="project",
    )(pieces, gain.reshape(tall, LANES), held, other, bias.reshape(1, H), max_state)


def renew(layer, pieces, product, first, carried, fresh, norm, mem, devices):
    last = first is not None
    args = [pieces, product] + ([first] if last else []) + [carried, fresh, norm, mem]
    return pl.pallas_call(
        functools.partial(state_kernel, layer=layer, last=last),
        out_shape=(f32(*mem.shape[1:]), bf16((4 if last else 2) * devices, LANES)),
        in_specs=[VMEM] * len(args),
        out_specs=[VMEM] * 2,
        scratch_shapes=[pltpu.VMEM((2 * SEQS, LANES), jnp.float32)],
        compiler_params=room(),
        cost_estimate=cost(1 << 23),
        name="renew_last" if last else "renew",
    )(*args)


def output(pieces, held, other, x):
    return pl.pallas_call(
        output_kernel,
        out_shape=(bf16(*x.shape), bf16(*pieces.shape)),
        in_specs=[VMEM] * 4,
        out_specs=[VMEM] * 2,
        scratch_shapes=[pltpu.VMEM((pieces.shape[0] // SEQS, SEQS, LANES), jnp.float32)],
        compiler_params=room(),
        cost_estimate=cost(1 << 23),
        name="output",
    )(pieces, held, other, x)


def final(pieces, held, other, x, gates, norm, maxima, states):
    half = pieces.shape[0] // 2
    return pl.pallas_call(
        final_kernel,
        out_shape=(
            bf16(*x.shape), f32(*norm.shape), f32(BLOCKS, SEQS, H), f32(BLOCKS, *states[0].shape)
        ),
        in_specs=[VMEM] * 13,
        out_specs=[HBM] * 4,
        scratch_shapes=[
            pltpu.VMEM((2 * half, LANES), jnp.float32),
            pltpu.VMEM((half, LANES), jnp.float32),
            pltpu.VMEM((half // SEQS, SEQS, LANES), jnp.float32),
            pltpu.VMEM(x.shape, jnp.bfloat16),
            pltpu.VMEM(norm.shape, jnp.float32),
            pltpu.SemaphoreType.DMA((3, BLOCKS)),
        ],
        compiler_params=room(),
        cost_estimate=cost(1 << 23),
        name="final",
    )(pieces, held, other, x, *gates[0], *gates[1], norm, *maxima, *states)


def head_groups():
    size = lax.axis_size("t")
    return [list(range(at, at + PER_HEAD)) for at in range(0, size, PER_HEAD)]


def turned_group():
    size = lax.axis_size("t")
    return [[(i + size // TURN) % size for i in range(size)]]


def to_all(sent, groups):
    size = len(groups[0])
    got = lax.all_to_all(
        sent.reshape(size, -1, LANES), "t", 0, 0, axis_index_groups=groups, tiled=True
    )
    return got.reshape(-1, LANES)


def rows_to_all(w):
    size = lax.axis_size("x")
    got = [lax.ppermute(w, "x", [(i, (i + k) % size) for i in range(size)]) for k in range(1, size)]
    held = jnp.stack([w, *got])
    other = lax.ppermute(held, "c", [(0, 1), (1, 0)])
    return held, other


def shards(
    tokens,
    norm_gain,
    w_query,
    w_key,
    w_value,
    w_outgate,
    w_ingate,
    w_forget,
    forget_bias,
    w_output,
    mem_state,
    norm_state,
    max_state,
):
    devices = lax.axis_size("t")
    projections = (w_query, w_key, w_value, w_outgate, w_ingate, w_forget)

    sent, lines = prepare(tokens, projections, w_output, devices)
    weights = rows_to_all(lines)
    current = tokens
    gates, maxima, states, first = ([], [], [], None)
    for layer in range(BLOCKS):
        pieces = to_all(sent, turned_group())
        sent, product, new_max, carried, fresh = project(
            layer, pieces, norm_gain[layer], *weights, forget_bias[layer], max_state[layer]
        )
        pieces = to_all(sent, head_groups())
        state, sent = renew(
            layer, pieces, product, first, carried, fresh, norm_state, mem_state, devices
        )
        first = product
        states.append(state)
        gates.append((carried, fresh))
        maxima.append(new_max)
        pieces = to_all(sent, turned_group())
        if layer < BLOCKS - 1:
            current, sent = output(pieces, *weights, current)
    current, new_norm, new_max, new_mem = final(
        pieces, *weights, current, gates, norm_state, maxima, states
    )
    return (current, new_mem, new_norm, new_max)


def solution(mesh):
    dp = ("x", "c")
    split = Mesh(
        mesh.devices.reshape(mesh.shape["tp"], mesh.shape["dp"] // 2, 2), ("t", "x", "c")
    )

    return jax.shard_map(
        shards,
        mesh=split,
        in_specs=(
            P(dp, "t"),
            P(),
            P(None, dp, "t"),
            P(None, dp, "t"),
            P(None, dp, "t"),
            P(None, dp, "t"),
            P(None, dp, None),
            P(None, dp, None),
            P(),
            P(None, dp, "t"),
            P(None, dp, "t", None),
            P(None, dp, None, None),
            P(None, dp, None),
        ),
        out_specs=(
            P(dp, "t"),
            P(None, dp, "t", None),
            P(None, dp, None, None),
            P(None, dp, None),
        ),
        check_vma=False,
    )
```
